512 devices in a mesh: grp: 2 (over y), tp: 32 (over z), dp: 8 (over x, core).
Axes of the slice: x: 4, y: 2, z: 32, core: 2. Of those that a mesh axis runs over, the one named last changes fastest.
The devices are a block of a 4x8x32 slice.
Arguments:
- tokens: bfloat16 [256, 4096], P('grp', 'dp'), parts along dimension 0, may hold values from -6 to 6
- norm_gain: float32 [2, 4096], P(None, 'dp'), may hold values from 0.1 to 1.9
- w_query: bfloat16 [2, 4096, 4096], P(None, 'dp', 'tp'), may hold values from -0.09375 to 0.09375
- w_key: bfloat16 [2, 4096, 4096], P(None, 'dp', 'tp'), may hold values from -0.09375 to 0.09375
- w_value: bfloat16 [2, 4096, 4096], P(None, 'dp', 'tp'), may hold values from -0.09375 to 0.09375
- w_outgate: bfloat16 [2, 4096, 4096], P(None, 'dp', 'tp'), may hold values from -0.09375 to 0.09375
- gate_weight: bfloat16 [2, 32, 384, 2], P(None, 'tp'), may hold values from -0.3125 to 0.3125
- forget_bias: float32 [2, 32], P(None, 'tp'), may hold values from -2 to 4
- w_mix: bfloat16 [2, 4096, 4096], P(None, 'tp', 'dp'), may hold values from -0.09375 to 0.09375
- memory: float32 [2, 256, 32, 128, 128], P(None, ('grp', 'dp'), 'tp'), parts along dimension 1, may hold values from -3 to 3
- normalizer: float32 [2, 256, 32, 128], P(None, ('grp', 'dp'), 'tp'), parts along dimension 1, may hold values from -3 to 3
- stabilizer: float32 [2, 256, 32], P(None, ('grp', 'dp'), 'tp'), parts along dimension 1, may hold values from -4 to 4
Outputs:
- result: bfloat16 [256, 4096], P('grp', 'dp'), parts along dimension 0
- new_memory: float32 [2, 256, 32, 128, 128], P(None, ('grp', 'dp'), 'tp'), parts along dimension 1
- new_normalizer: float32 [2, 256, 32, 128], P(None, ('grp', 'dp'), 'tp'), parts along dimension 1
- new_stabilizer: float32 [2, 256, 32], P(None, ('grp', 'dp'), 'tp'), parts along dimension 1
The draws below stay inside these ranges and needn't reach their ends.
There are 2 independent parts, one for each index of `grp`. The reference program is written for one: setup_inputs(seed, part) draws one part's arguments, and reference() takes and returns one part's arrays. A program takes and returns all parts, laid end to end along the dimension named above; an argument that names none is the same for every part. Nothing has to cross between parts.
All inputs are finite; a program needn't handle non-finite values.
Results may differ from the reference program's by a relative error of at most 0.018.
Values may be sent and summed in bfloat16 or wider, within the bound.
A program may use at most 64 MiB of HBM per device.

```python
import jax
import jax.numpy as jnp
from jax import lax

D = 4096
DK = 128
BLOCKS = 2
HEADS = 32
INNER = 4096
SEQS = 128


def shard_levels(key, shape, cuts, least, top_value):
    factor_of, own = 1.0, jax.random.fold_in(key, 6)
    for axis_at, parts in cuts:
        steps = jnp.exp(jax.random.uniform(jax.random.fold_in(own, axis_at), (parts,), jnp.float32, least / len(cuts), top_value / len(cuts)))
        factor_of = factor_of * jnp.repeat(steps, shape[axis_at] // parts).reshape([-1 if axis == axis_at else 1 for axis in range(len(shape))])
    return factor_of


def gaussian(stream_key, dims, spread, reach, shards=(), kind=jnp.bfloat16):
    loudness = shard_levels(stream_key, dims, shards, -0.22, 0.18) if shards else 1.0
    entries = jax.random.normal(stream_key, dims, jnp.float32) * spread * loudness
    return jnp.minimum(jnp.maximum(entries, -reach), reach).astype(kind)


def setup_inputs(seed: int = 0, part: int = 0) -> dict:
    key_list = jax.random.split(jax.random.key(seed), 13)
    part_splits = jax.random.split(jax.random.fold_in(key_list[12], part), 13)
    tokens = gaussian(part_splits[0], (SEQS, D), 1.0, 6.0, ((1, 8),))
    norm_gain = jnp.clip(1.0 + 0.18 * jax.random.normal(key_list[1], (BLOCKS, D), jnp.float32), 0.1, 1.9)
    w_query = gaussian(key_list[2], (BLOCKS, D, INNER), D ** -0.5, 0.09375, ((1, 8), (2, 32)))
    w_key = gaussian(key_list[3], (BLOCKS, D, INNER), D ** -0.5, 0.09375, ((1, 8), (2, 32)))
    w_value = gaussian(key_list[4], (BLOCKS, D, INNER), D ** -0.5, 0.09375, ((1, 8), (2, 32)))
    w_outgate = gaussian(key_list[5], (BLOCKS, D, INNER), D ** -0.5, 0.09375, ((1, 8), (2, 32)))
    gate_weight = gaussian(key_list[6], (BLOCKS, HEADS, 3 * DK, 2), (3 * DK) ** -0.5, 0.3125, ((1, 32),))
    forget_bias = jnp.clip(-2.0 + 6.0 * jax.random.uniform(key_list[7], (BLOCKS, HEADS), jnp.float32) ** shard_levels(key_list[7], (BLOCKS, HEADS), ((1, 32),), -0.2, 0.2), -2.0, 4.0)
    w_mix = gaussian(key_list[8], (BLOCKS, INNER, D), INNER ** -0.5, 0.09375, ((1, 32), (2, 8)))
    memory = gaussian(part_splits[9], (BLOCKS, SEQS, HEADS, DK, DK), 0.3, 3.0, ((1, 8), (2, 32)), jnp.float32)
    normalizer = gaussian(part_splits[10], (BLOCKS, SEQS, HEADS, DK), 0.3, 3.0, ((1, 8), (2, 32)), jnp.float32)
    stabilizer = gaussian(part_splits[11], (BLOCKS, SEQS, HEADS), 1.0, 4.0, ((1, 8), (2, 32)), jnp.float32)
    return dict(tokens=tokens, norm_gain=norm_gain, w_query=w_query, w_key=w_key, w_value=w_value, w_outgate=w_outgate, gate_weight=gate_weight, forget_bias=forget_bias, w_mix=w_mix, memory=memory, normalizer=normalizer, stabilizer=stabilizer)


EPS = 1e-06

def reference(tokens, norm_gain, w_query, w_key, w_value, w_outgate, gate_weight, forget_bias, w_mix, memory, normalizer, stabilizer):
    x = tokens
    mems, norms, stabs = ([], [], [])
    seqs = tokens.shape[0]
    for blk in range(BLOCKS):
        xf = x.astype(jnp.float32)
        squares = lax.optimization_barrier(jnp.sum(xf * xf, axis=-1))
        scale = lax.rsqrt(squares / D + EPS)
        scaled_in = (xf * norm_gain[blk]).astype(jnp.bfloat16)
        projs = []
        for weight in (w_query, w_key, w_value, w_outgate):
            prod = jnp.dot(scaled_in, weight[blk], preferred_element_type=jnp.float32)
            projs.append((scale[:, None] * prod).astype(jnp.bfloat16).astype(jnp.float32).reshape(seqs, HEADS, DK))
        query, key, value, outgate = projs
        joined = jnp.concatenate([query, key, value], axis=-1)
        pre = jnp.einsum('shc,hcg->shg', joined, gate_weight[blk].astype(jnp.float32), precision=lax.Precision.HIGHEST)
        log_input = pre[..., 0]
        log_forget = jax.nn.log_sigmoid(pre[..., 1] + forget_bias[blk])
        stab = stabilizer[blk]
        new_stab = jnp.maximum(log_forget + stab, log_input)
        keep = jnp.exp(log_forget + stab - new_stab)
        admit = jnp.exp(log_input - new_stab)
        scaled_key = key * DK ** (-0.5)
        new_mem = keep[..., None, None] * memory[blk] + admit[..., None, None] * scaled_key[..., :, None] * value[..., None, :]
        new_norm = keep[..., None] * normalizer[blk] + admit[..., None] * scaled_key
        numer = jnp.einsum('shd,shde->she', query, new_mem, precision=lax.Precision.HIGHEST)
        denom = jnp.maximum(jnp.abs(lax.optimization_barrier(jnp.sum(query * new_norm, axis=-1))), 1.0)
        readout = numer / denom[..., None]
        gated = (readout * jax.nn.sigmoid(outgate)).reshape(seqs, HEADS * DK).astype(jnp.bfloat16)
        mixed = jnp.dot(gated, w_mix[blk], preferred_element_type=jnp.float32)
        x = (xf + mixed).astype(jnp.bfloat16)
        mems.append(new_mem)
        norms.append(new_norm)
        stabs.append(new_stab)
    return (x, jnp.stack(mems, axis=0), jnp.stack(norms, axis=0), jnp.stack(stabs, axis=0))
```

```python
import functools

import jax
import jax.numpy as jnp
from jax import lax
from jax.experimental import pallas as pl
from jax.experimental.pallas import tpu as pltpu
from jax.sharding import PartitionSpec as P

EPS = 1e-06
MESH = pl.DeviceIdType.MESH
NEAR = 8
EXTRA = 128
ANY = pl.BlockSpec(memory_space=pl.ANY)
VM = pl.BlockSpec(memory_space=pltpu.VMEM)


def ahead_first(count):
    return sorted(range(1, count), key=lambda k: -min(k, count - k))


def step_kernel(
    n_dp, n_tp, dims,
    tokens, gain, wq, wk, wv, wo, gate_w, bias, wmix, memory, norm, stab,
    x_out, vec_out,
    xbuf, wbuf, mixbuf, membuf, part, send1, recv1, gath, mixpart, send3, recv3, far,
    load_sem, s1, r1, s2, r2, s3, r3, s4, r4, s5, r5,
):
    blocks, rows, feats, dk, model = dims
    cols = 4 * dk
    dp, tp = lax.axis_index("dp"), lax.axis_index("tp")
    n_far = n_tp // NEAR
    group, j = tp // NEAR, lax.rem(tp, NEAR)

    def at_dp(k):
        return {"dp": lax.rem(dp + k, n_dp)}

    def at_near(k):
        return {"tp": group * NEAR + lax.rem(j + k, NEAR)}

    def at_tp(k):
        return {"tp": lax.rem(tp + k + n_tp, n_tp)}

    window = sorted(range(-(NEAR // 2) + 1, NEAR // 2 + 1), key=lambda k: -abs(k))
    window = [k for k in window if k]

    barrier = pltpu.get_barrier_semaphore()
    peers = [at_tp(NEAR * k) for k in ahead_first(n_far)]
    peers += [at_near(k) for k in ahead_first(NEAR)]
    peers += [at_tp(k) for h in range(1, NEAR // 2 + 1) for k in (h, -h)]
    peers += [at_dp(k) for k in ahead_first(n_dp)]
    for peer in peers:
        pl.semaphore_signal(barrier, inc=1, device_id=peer, device_id_type=MESH)

    loads = []

    def load(src, dst):
        copy = pltpu.make_async_copy(src, dst, load_sem.at[len(loads)])
        copy.start()
        loads.append(copy)
        return copy

    w_loads, mix_loads, mem_loads = [], [], []
    for b in range(blocks):
        w_loads.append(
            [load(w.at[b], wbuf.at[b, :, pl.ds(i * dk, dk)]) for i, w in enumerate((wq, wk, wv, wo))]
        )
        mem_loads.append(load(memory.at[b, :, 0], membuf.at[b]))
        mix_loads.append(load(wmix.at[b], mixbuf.at[b]))

    pl.semaphore_wait(barrier, len(peers))

    def rows_of(block):
        return pl.ds(pl.multiple_of(block * rows, rows), rows)

    sent = []

    def push(src, dst, send, recv, peer):
        copy = pltpu.make_async_remote_copy(
            src_ref=src, dst_ref=dst, send_sem=send, recv_sem=recv,
            device_id=peer, device_id_type=MESH,
        )
        copy.start()
        sent.append(copy)
        return copy

    for b in range(blocks):
        x_now = tokens if b == 0 else xbuf.at[b - 1]
        xf = x_now[...].astype(jnp.float32)
        scaled_in = (xf * gain[b : b + 1, :]).astype(jnp.bfloat16)
        squares = jnp.sum(xf * xf, axis=-1, keepdims=True)
        high = squares.astype(jnp.bfloat16).astype(jnp.float32)
        lane = lax.broadcasted_iota(jnp.int32, (xf.shape[0], EXTRA), 1)
        tail = jnp.where(lane == 0, high, jnp.where(lane == 1, squares - high, 0.0))
        send1[b, :, cols:] = tail.astype(jnp.bfloat16)
        for copy in w_loads[b]:
            copy.wait()
        prod = jnp.dot(scaled_in, wbuf[b], preferred_element_type=jnp.float32)
        part[...] = prod
        send1[b, :, :cols] = prod.astype(jnp.bfloat16)
        copies = [
            push(send1.at[b, rows_of(lax.rem(dp + k, n_dp))], recv1.at[b, k - 1],
                 s1.at[b, k - 1], r1.at[b, k - 1], at_dp(k))
            for k in ahead_first(n_dp)
        ]
        total = part[rows_of(dp), :]
        own_tail = send1[b, rows_of(dp), cols:].astype(jnp.float32)
        for copy in copies:
            copy.wait_recv()
        for k in range(1, n_dp):
            total = total + recv1[b, k - 1, :, :cols].astype(jnp.float32)
            own_tail = own_tail + recv1[b, k - 1, :, cols:].astype(jnp.float32)
        all_squares = jnp.sum(own_tail, axis=-1, keepdims=True)
        scale = lax.rsqrt(all_squares / model + EPS)
        proj = (scale * total).astype(jnp.bfloat16)
        query, key, value, outgate = (
            proj[:, i * dk : (i + 1) * dk].astype(jnp.float32) for i in range(4)
        )
        pre = jnp.dot(proj[:, : 3 * dk], gate_w[b, 0], preferred_element_type=jnp.float32)
        log_input = pre[:, 0:1]
        shifted = pre[:, 1:2] + bias[b : b + 1, 0:1]
        log_forget = jnp.minimum(shifted, 0.0) - jnp.log1p(jnp.exp(-jnp.abs(shifted)))
        old = stab[b]
        new_stab = jnp.maximum(log_forget + old, log_input)
        keep = jnp.exp(log_forget + old - new_stab)
        admit = jnp.exp(log_input - new_stab)
        scaled_key = key * dk ** (-0.5)
        admitted = admit * scaled_key
        new_norm = keep * norm[b, :, 0] + admitted
        mem_loads[b].wait()
        query_t = query.T
        recalled = jnp.concatenate(
            [
                jnp.sum(query_t[:, s : s + 1] * membuf[b, s], axis=0, keepdims=True)
                for s in range(rows)
            ],
            axis=0,
        )
        match = jnp.sum(query * admitted, axis=-1, keepdims=True)
        numer = keep * recalled + match * value
        denom = jnp.maximum(jnp.abs(jnp.sum(query * new_norm, axis=-1, keepdims=True)), 1.0)
        gated = numer / denom * jax.nn.sigmoid(outgate)
        gath[b, rows_of(dp), :] = gated.astype(jnp.bfloat16)
        copies = [
            push(gath.at[b, rows_of(dp)], gath.at[b, rows_of(dp)],
                 s2.at[b, k - 1], r2.at[b, k - 1], at_dp(k))
            for k in ahead_first(n_dp)
        ]
        vec_out[b, 0] = jnp.broadcast_to(keep, (rows, dk))
        vec_out[b, 1] = admitted
        vec_out[b, 2] = value
        vec_out[b, 3] = new_norm
        vec_out[b, 4] = jnp.broadcast_to(new_stab, (rows, dk))
        mix_loads[b].wait()
        for copy in copies:
            copy.wait_recv()
        prod = jnp.dot(gath[b], mixbuf[b], preferred_element_type=jnp.float32)
        mixpart[...] = prod
        send3[b] = prod.astype(jnp.bfloat16)
        copies = [
            push(send3.at[b, rows_of(lax.rem(j + k, NEAR))], recv3.at[b, k - 1],
                 s3.at[b, k - 1], r3.at[b, k - 1], at_near(k))
            for k in ahead_first(NEAR)
        ]
        total = mixpart[rows_of(j), :]
        for copy in copies:
            copy.wait_recv()
        for k in range(1, NEAR):
            total = total + recv3[b, k - 1].astype(jnp.float32)
        far[b, group] = total.astype(jnp.bfloat16)
        copies = [
            push(far.at[b, group], far.at[b, group], s4.at[b, k - 1], r4.at[b, k - 1], at_tp(NEAR * k))
            for k in ahead_first(n_far)
        ]
        total = x_now[rows_of(j), :].astype(jnp.float32)
        for copy in copies:
            copy.wait_recv()
        mixed = far[b, 0].astype(jnp.float32)
        for k in range(1, n_far):
            mixed = mixed + far[b, k].astype(jnp.float32)
        xbuf[b, rows_of(j), :] = (total + mixed).astype(jnp.bfloat16)
        copies = [
            push(xbuf.at[b, rows_of(j)], xbuf.at[b, rows_of(j)], s5.at[b, i], r5.at[b, i], at_tp(k))
            for i, k in enumerate(window)
        ]
        for copy in copies:
            copy.wait_recv()
    x_out[...] = xbuf[blocks - 1]
    for copy in sent:
        copy.wait_send()


def finish_kernel(rows, x, vec, memory, x_out, mem_out, norm_out, stab_out):
    admitted_t = vec[0, 1].T
    for s in range(rows):
        mem_out[0, s, 0] = (
            vec[0, 0, s : s + 1, :] * memory[0, s, 0]
            + admitted_t[:, s : s + 1] * vec[0, 2, s : s + 1, :]
        )
    norm_out[0, :, 0] = vec[0, 3]
    stab_out[0] = vec[0, 4, :, 0:1]
    x_out[...] = x[...]


def shards(n_dp, n_tp, *args):
    tokens, gain, wq, wk, wv, wo, gate_w, bias, wmix, memory, norm, stab = args
    blocks, rows, _, dk, _ = memory.shape
    seqs, feats = tokens.shape
    n_far = n_tp // NEAR
    dims = (blocks, rows, feats, dk, feats * n_dp)
    bf, f32 = jnp.bfloat16, jnp.float32
    dma = pltpu.SemaphoreType.DMA
    x, vec = pl.pallas_call(
        functools.partial(step_kernel, n_dp, n_tp, dims),
        out_shape=(
            jax.ShapeDtypeStruct((seqs, feats), bf),
            jax.ShapeDtypeStruct((blocks, 5, rows, dk), f32),
        ),
        in_specs=[VM, VM, ANY, ANY, ANY, ANY, VM, VM, ANY, ANY, VM, VM],
        out_specs=(VM, VM),
        scratch_shapes=[
            pltpu.VMEM((blocks, seqs, feats), bf),
            pltpu.VMEM((blocks, feats, 4 * dk), bf),
            pltpu.VMEM((blocks, dk, feats), bf),
            pltpu.VMEM((blocks, rows, dk, dk), f32),
            pltpu.VMEM((seqs, 4 * dk), f32),
            pltpu.VMEM((blocks, seqs, 4 * dk + EXTRA), bf),
            pltpu.VMEM((blocks, n_dp - 1, rows, 4 * dk + EXTRA), bf),
            pltpu.VMEM((blocks, seqs, dk), bf),
            pltpu.VMEM((seqs, feats), f32),
            pltpu.VMEM((blocks, seqs, feats), bf),
            pltpu.VMEM((blocks, NEAR - 1, rows, feats), bf),
            pltpu.VMEM((blocks, n_far, rows, feats), bf),
            dma((blocks * 6,)),
            dma((blocks, n_dp - 1)),
            dma((blocks, n_dp - 1)),
            dma((blocks, n_dp - 1)),
            dma((blocks, n_dp - 1)),
            dma((blocks, NEAR - 1)),
            dma((blocks, NEAR - 1)),
            dma((blocks, n_far - 1)),
            dma((blocks, n_far - 1)),
            dma((blocks, NEAR - 1)),
            dma((blocks, NEAR - 1)),
        ],
        compiler_params=pltpu.CompilerParams(collective_id=0, has_side_effects=True),
        name="two_cells",
    )(*args)
    return tuple(
        pl.pallas_call(
            functools.partial(finish_kernel, rows),
            grid=(blocks,),
            out_shape=(
                jax.ShapeDtypeStruct((seqs, feats), bf),
                jax.ShapeDtypeStruct(memory.shape, f32),
                jax.ShapeDtypeStruct(norm.shape, f32),
                jax.ShapeDtypeStruct(stab.shape, f32),
            ),
            in_specs=[
                pl.BlockSpec((seqs, feats), lambda b: (0, 0)),
                pl.BlockSpec((1, 5, rows, dk), lambda b: (b, 0, 0, 0)),
                pl.BlockSpec((1, rows, 1, dk, dk), lambda b: (b, 0, 0, 0, 0)),
            ],
            out_specs=(
                pl.BlockSpec((seqs, feats), lambda b: (0, 0)),
                pl.BlockSpec((1, rows, 1, dk, dk), lambda b: (b, 0, 0, 0, 0)),
                pl.BlockSpec((1, rows, 1, dk), lambda b: (b, 0, 0, 0)),
                pl.BlockSpec((1, rows, 1), lambda b: (b, 0, 0)),
            ),
            name="finish",
        )(x, vec, memory)
    )


def solution(mesh):
    in_specs = (
        P("grp", "dp"),
        P(None, "dp"),
        P(None, "dp", "tp"),
        P(None, "dp", "tp"),
        P(None, "dp", "tp"),
        P(None, "dp", "tp"),
        P(None, "tp", None, None),
        P(None, "tp"),
        P(None, "tp", "dp"),
        P(None, ("grp", "dp"), "tp", None, None),
        P(None, ("grp", "dp"), "tp", None),
        P(None, ("grp", "dp"), "tp"),
    )
    out_specs = (
        P("grp", "dp"),
        P(None, ("grp", "dp"), "tp", None, None),
        P(None, ("grp", "dp"), "tp", None),
        P(None, ("grp", "dp"), "tp"),
    )
    body = functools.partial(shards, mesh.shape["dp"], mesh.shape["tp"])
    return jax.shard_map(body, mesh=mesh, in_specs=in_specs, out_specs=out_specs, check_vma=False)
```

```python
import functools

import jax
import jax.numpy as jnp
from jax import lax
from jax.experimental import pallas as pl
from jax.experimental.pallas import tpu as pltpu
from jax.sharding import PartitionSpec as P

EPS = 1e-06
MESH = pl.DeviceIdType.MESH
NEAR = 8
EXTRA = 128
ANY = pl.BlockSpec(memory_space=pl.ANY)
VM = pl.BlockSpec(memory_space=pltpu.VMEM)


def ahead_first(count):
    return sorted(range(1, count), key=lambda k: -min(k, count - k))


def eye(n):
    return lax.broadcasted_iota(jnp.int32, (n, n), 0) == lax.broadcasted_iota(jnp.int32, (n, n), 1)


def step_kernel(
    n_dp, n_tp, dims,
    tokens, gain, wq, wk, wv, wo, gate_w, bias, wmix, memory, norm, stab,
    x_out, vec_out,
    xbuf, wbuf, mixbuf, membuf, part, send1, recv1, gath, mixpart, send3, recv3, far,
    load_sem, token, s1, r1, s2, r2, s3, r3, s4, r4, s5, r5,
):
    blocks, rows, feats, dk, model = dims
    cols = 4 * dk
    dp, tp = lax.axis_index("dp"), lax.axis_index("tp")
    n_far = n_tp // NEAR
    group, j = tp // NEAR, lax.rem(tp, NEAR)

    def at_dp(k):
        return {"dp": lax.rem(dp + k, n_dp)}

    def at_near(k):
        return {"tp": group * NEAR + lax.rem(j + k, NEAR)}

    def at_tp(k):
        return {"tp": lax.rem(tp + k + n_tp, n_tp)}

    window = sorted(range(-(NEAR // 2) + 1, NEAR // 2 + 1), key=lambda k: -abs(k))
    window = [k for k in window if k]

    barrier = pltpu.get_barrier_semaphore()
    circles = [
        [at_near(k) for k in ahead_first(NEAR)],
        [at_tp(NEAR * k) for k in ahead_first(n_far)],
        [at_tp(k) for h in range(1, NEAR // 2 + 1) for k in (h, -h)],
    ]
    for k in ahead_first(n_dp):
        pl.semaphore_signal(barrier, inc=1, device_id=at_dp(k), device_id_type=MESH)
    lower, higher = jnp.int32(n_dp - 1), []
    for circle in circles:
        above = jnp.int32(0)
        for peer in circle:

            @pl.when(peer["tp"] > tp)
            def _(peer=peer):
                pl.semaphore_signal(barrier, inc=1, device_id=peer, device_id_type=MESH)

            above = above + jnp.where(peer["tp"] > tp, 1, 0)
        lower = lower + (len(circle) - above)
        higher.append(above)

    loads = []

    def load(src, dst):
        copy = pltpu.make_async_copy(src, dst, load_sem.at[len(loads)])
        copy.start()
        loads.append(copy)
        return copy

    w_loads, mix_loads, mem_loads = [], [], []
    for b in range(blocks):
        w_loads.append(
            [load(w.at[b], wbuf.at[b, :, pl.ds(i * dk, dk)]) for i, w in enumerate((wq, wk, wv, wo))]
        )
        mem_loads.append(load(memory.at[b, :, 0], membuf.at[b]))
        mix_loads.append(load(wmix.at[b], mixbuf.at[b]))

    pl.semaphore_wait(barrier, lower)
    for i, circle in enumerate(circles):
        for peer in circle:

            @pl.when(peer["tp"] < tp)
            def _(peer=peer, i=i):
                pl.semaphore_signal(token.at[i], inc=1, device_id=peer, device_id_type=MESH)

    def met(b, i):
        if b == 0:

            @pl.when(higher[i] > 0)
            def _():
                pl.semaphore_wait(token.at[i], higher[i])

    def rows_of(block):
        return pl.ds(pl.multiple_of(block * rows, rows), rows)

    sent = []

    def push(src, dst, send, recv, peer):
        copy = pltpu.make_async_remote_copy(
            src_ref=src, dst_ref=dst, send_sem=send, recv_sem=recv,
            device_id=peer, device_id_type=MESH,
        )
        copy.start()
        sent.append(copy)
        return copy

    for b in range(blocks):
        x_now = tokens if b == 0 else xbuf.at[b - 1]
        xf = x_now[...].astype(jnp.float32)
        scaled_in = (xf * gain[b : b + 1, :]).astype(jnp.bfloat16)
        squares = jnp.sum(xf * xf, axis=-1, keepdims=True)
        high = squares.astype(jnp.bfloat16).astype(jnp.float32)
        lane = lax.broadcasted_iota(jnp.int32, (xf.shape[0], EXTRA), 1)
        tail = jnp.where(lane == 0, high, jnp.where(lane == 1, squares - high, 0.0))
        send1[b, :, cols:] = tail.astype(jnp.bfloat16)
        for copy in w_loads[b]:
            copy.wait()
        prod = jnp.dot(scaled_in, wbuf[b], preferred_element_type=jnp.float32)
        part[...] = prod
        send1[b, :, :cols] = prod.astype(jnp.bfloat16)
        copies = [
            push(send1.at[b, rows_of(lax.rem(dp + k, n_dp))], recv1.at[b, k - 1],
                 s1.at[b, k - 1], r1.at[b, k - 1], at_dp(k))
            for k in ahead_first(n_dp)
        ]
        total = part[rows_of(dp), :]
        own_tail = send1[b, rows_of(dp), cols:].astype(jnp.float32)
        for copy in copies:
            copy.wait_recv()
        for k in range(1, n_dp):
            total = total + recv1[b, k - 1, :, :cols].astype(jnp.float32)
            own_tail = own_tail + recv1[b, k - 1, :, cols:].astype(jnp.float32)
        all_squares = jnp.sum(own_tail, axis=-1, keepdims=True)
        scale = lax.rsqrt(all_squares / model + EPS)
        proj = (scale * total).astype(jnp.bfloat16)
        query, key, value, outgate = (
            proj[:, i * dk : (i + 1) * dk].astype(jnp.float32) for i in range(4)
        )
        pre = lax.dot_general(
            proj[:, : 3 * dk], gate_w[b, 0], (((1,), (1,)), ((), ())), preferred_element_type=jnp.float32
        )
        log_input = pre[:, 0:1]
        shifted = pre[:, 1:2] + bias[:, b : b + 1]
        log_forget = jnp.minimum(shifted, 0.0) - jnp.log1p(jnp.exp(-jnp.abs(shifted)))
        old = jnp.sum(jnp.where(eye(rows), stab[b], 0.0), axis=1, keepdims=True)
        new_stab = jnp.maximum(log_forget + old, log_input)
        keep = jnp.exp(log_forget + old - new_stab)
        admit = jnp.exp(log_input - new_stab)
        scaled_key = key * dk ** (-0.5)
        admitted = admit * scaled_key
        new_norm = keep * norm[b, :, 0] + admitted
        mem_loads[b].wait()
        query_t = query.T
        recalled = jnp.concatenate(
            [
                jnp.sum(query_t[:, s : s + 1] * membuf[b, s], axis=0, keepdims=True)
                for s in range(rows)
            ],
            axis=0,
        )
        match = jnp.sum(query * admitted, axis=-1, keepdims=True)
        numer = keep * recalled + match * value
        denom = jnp.maximum(jnp.abs(jnp.sum(query * new_norm, axis=-1, keepdims=True)), 1.0)
        gated = numer / denom * jax.nn.sigmoid(outgate)
        gath[b, rows_of(dp), :] = gated.astype(jnp.bfloat16)
        copies = [
            push(gath.at[b, rows_of(dp)], gath.at[b, rows_of(dp)],
                 s2.at[b, k - 1], r2.at[b, k - 1], at_dp(k))
            for k in ahead_first(n_dp)
        ]
        vec_out[b, 0] = jnp.broadcast_to(keep, (rows, dk))
        vec_out[b, 1] = admitted
        vec_out[b, 2] = value
        vec_out[b, 3] = new_norm
        vec_out[b, 4] = jnp.broadcast_to(new_stab, (rows, dk))
        mix_loads[b].wait()
        for copy in copies:
            copy.wait_recv()
        prod = jnp.dot(gath[b], mixbuf[b], preferred_element_type=jnp.float32)
        mixpart[...] = prod
        send3[b] = prod.astype(jnp.bfloat16)
        met(b, 0)
        copies = [
            push(send3.at[b, rows_of(lax.rem(j + k, NEAR))], recv3.at[b, k - 1],
                 s3.at[b, k - 1], r3.at[b, k - 1], at_near(k))
            for k in ahead_first(NEAR)
        ]
        total = mixpart[rows_of(j), :]
        for copy in copies:
            copy.wait_recv()
        for k in range(1, NEAR):
            total = total + recv3[b, k - 1].astype(jnp.float32)
        far[b, group] = total.astype(jnp.bfloat16)
        met(b, 1)
        copies = [
            push(far.at[b, group], far.at[b, group], s4.at[b, k - 1], r4.at[b, k - 1], at_tp(NEAR * k))
            for k in ahead_first(n_far)
        ]
        total = x_now[rows_of(j), :].astype(jnp.float32)
        for copy in copies:
            copy.wait_recv()
        mixed = far[b, 0].astype(jnp.float32)
        for k in range(1, n_far):
            mixed = mixed + far[b, k].astype(jnp.float32)
        xbuf[b, rows_of(j), :] = (total + mixed).astype(jnp.bfloat16)
        met(b, 2)
        copies = [
            push(xbuf.at[b, rows_of(j)], xbuf.at[b, rows_of(j)], s5.at[b, i], r5.at[b, i], at_tp(k))
            for i, k in enumerate(window)
        ]
        for copy in copies:
            copy.wait_recv()
    x_out[...] = xbuf[blocks - 1]
    for copy in sent:
        copy.wait_send()


def finish_kernel(rows, x, vec, memory, x_out, mem_out, norm_out, stab_out):
    admitted_t = vec[0, 1].T
    for s in range(rows):
        mem_out[0, s, 0] = (
            vec[0, 0, s : s + 1, :] * memory[0, s, 0]
            + admitted_t[:, s : s + 1] * vec[0, 2, s : s + 1, :]
        )
    norm_out[0, :, 0] = vec[0, 3]
    stab_out[0] = jnp.sum(jnp.where(eye(rows), vec[0, 4, :, :rows], 0.0), axis=0, keepdims=True)
    x_out[...] = x[...]


def shards(n_dp, n_tp, *args):
    tokens, gain, wq, wk, wv, wo, gate_w, bias, wmix, memory, norm, stab = args
    blocks, rows, _, dk, _ = memory.shape
    seqs, feats = tokens.shape
    n_far = n_tp // NEAR
    dims = (blocks, rows, feats, dk, feats * n_dp)
    bf, f32 = jnp.bfloat16, jnp.float32
    gate_w, bias, stab = gate_w.transpose(0, 1, 3, 2), bias.T, stab.transpose(0, 2, 1)
    dma = pltpu.SemaphoreType.DMA
    x, vec = pl.pallas_call(
        functools.partial(step_kernel, n_dp, n_tp, dims),
        out_shape=(
            jax.ShapeDtypeStruct((seqs, feats), bf),
            jax.ShapeDtypeStruct((blocks, 5, rows, dk), f32),
        ),
        in_specs=[VM, VM, ANY, ANY, ANY, ANY, VM, VM, ANY, ANY, VM, VM],
        out_specs=(VM, VM),
        scratch_shapes=[
            pltpu.VMEM((blocks, seqs, feats), bf),
            pltpu.VMEM((blocks, feats, 4 * dk), bf),
            pltpu.VMEM((blocks, dk, feats), bf),
            pltpu.VMEM((blocks, rows, dk, dk), f32),
            pltpu.VMEM((seqs, 4 * dk), f32),
            pltpu.VMEM((blocks, seqs, 4 * dk + EXTRA), bf),
            pltpu.VMEM((blocks, n_dp - 1, rows, 4 * dk + EXTRA), bf),
            pltpu.VMEM((blocks, seqs, dk), bf),
            pltpu.VMEM((seqs, feats), f32),
            pltpu.VMEM((blocks, seqs, feats), bf),
            pltpu.VMEM((blocks, NEAR - 1, rows, feats), bf),
            pltpu.VMEM((blocks, n_far, rows, feats), bf),
            dma((blocks * 6,)),
            pltpu.SemaphoreType.REGULAR((3,)),
            dma((blocks, n_dp - 1)),
            dma((blocks, n_dp - 1)),
            dma((blocks, n_dp - 1)),
            dma((blocks, n_dp - 1)),
            dma((blocks, NEAR - 1)),
            dma((blocks, NEAR - 1)),
            dma((blocks, n_far - 1)),
            dma((blocks, n_far - 1)),
            dma((blocks, NEAR - 1)),
            dma((blocks, NEAR - 1)),
        ],
        compiler_params=pltpu.CompilerParams(collective_id=0, has_side_effects=True),
        name="two_cells",
    )(tokens, gain, wq, wk, wv, wo, gate_w, bias, wmix, memory, norm, stab)
    x, new_memory, new_norm, new_stab = pl.pallas_call(
        functools.partial(finish_kernel, rows),
        grid=(blocks,),
        out_shape=(
            jax.ShapeDtypeStruct((seqs, feats), bf),
            jax.ShapeDtypeStruct(memory.shape, f32),
            jax.ShapeDtypeStruct(norm.shape, f32),
            jax.ShapeDtypeStruct(stab.shape, f32),
        ),
        in_specs=[
            pl.BlockSpec((seqs, feats), lambda b: (0, 0)),
            pl.BlockSpec((1, 5, rows, dk), lambda b: (b, 0, 0, 0)),
            pl.BlockSpec((1, rows, 1, dk, dk), lambda b: (b, 0, 0, 0, 0)),
        ],
        out_specs=(
            pl.BlockSpec((seqs, feats), lambda b: (0, 0)),
            pl.BlockSpec((1, rows, 1, dk, dk), lambda b: (b, 0, 0, 0, 0)),
            pl.BlockSpec((1, rows, 1, dk), lambda b: (b, 0, 0, 0)),
            pl.BlockSpec((1, 1, rows), lambda b: (b, 0, 0)),
        ),
        name="finish",
    )(x, vec, memory)
    return x, new_memory, new_norm, new_stab.transpose(0, 2, 1)


def solution(mesh):
    in_specs = (
        P("grp", "dp"),
        P(None, "dp"),
        P(None, "dp", "tp"),
        P(None, "dp", "tp"),
        P(None, "dp", "tp"),
        P(None, "dp", "tp"),
        P(None, "tp", None, None),
        P(None, "tp"),
        P(None, "tp", "dp"),
        P(None, ("grp", "dp"), "tp", None, None),
        P(None, ("grp", "dp"), "tp", None),
        P(None, ("grp", "dp"), "tp"),
    )
    out_specs = (
        P("grp", "dp"),
        P(None, ("grp", "dp"), "tp", None, None),
        P(None, ("grp", "dp"), "tp", None),
        P(None, ("grp", "dp"), "tp"),
    )
    body = functools.partial(shards, mesh.shape["dp"], mesh.shape["tp"])
    return jax.shard_map(body, mesh=mesh, in_specs=in_specs, out_specs=out_specs, check_vma=False)
```

```python
import functools

import jax
import jax.numpy as jnp
from jax import lax
from jax.experimental import pallas as pl
from jax.experimental.pallas import tpu as pltpu
from jax.sharding import PartitionSpec as P

EPS = 1e-06
MESH = pl.DeviceIdType.MESH
NEAR = 8
EXTRA = 128
HBM = pl.BlockSpec(memory_space=pltpu.HBM)
VM = pl.BlockSpec(memory_space=pltpu.VMEM)


def ahead_first(count):
    return sorted(range(1, count), key=lambda k: -min(k, count - k))


def eye(n):
    return lax.broadcasted_iota(jnp.int32, (n, n), 0) == lax.broadcasted_iota(jnp.int32, (n, n), 1)


def step_kernel(
    n_dp, n_tp, dims,
    tokens_in, gain_in, wq, wk, wv, wo, gate_in, bias_in, wmix, memory, norm_in, stab_in,
    x_out, vec_out,
    tokens, gain, gate_w, bias, norm, stab, xbuf, wbuf, mixbuf, membuf, part, send1, recv1, gath, mixpart, send3, recv3, far,
    load_sem, token, s1, r1, s2, r2, s3, r3, s4, r4, s5, r5,
):
    blocks, rows, feats, dk, model = dims
    cols = 4 * dk
    dp, tp = lax.axis_index("dp"), lax.axis_index("tp")
    n_far = n_tp // NEAR
    group, j = tp // NEAR, lax.rem(tp, NEAR)

    def at_dp(k):
        return {"dp": lax.rem(dp + k, n_dp)}

    def at_tp(k):
        return {"tp": lax.rem(tp + k + n_tp, n_tp)}

    window = sorted(range(-(NEAR // 2) + 1, NEAR // 2 + 1), key=lambda k: -abs(k))
    window = [k for k in window if k]

    barrier = pltpu.get_barrier_semaphore()
    circles = [
        [at_tp(k) for h in range(NEAR // 2, 0, -1) for k in (h, -h)],
        [at_tp(NEAR * k) for k in ahead_first(n_far)],
    ]

    def rank(at):
        return jnp.where((at == 0) & (dp == 0), n_tp, at)

    own_rank = rank(tp)
    for k in ahead_first(n_dp):
        pl.semaphore_signal(barrier, inc=1, device_id=at_dp(k), device_id_type=MESH)
    lower, higher = jnp.int32(n_dp - 1), []
    for circle in circles:
        above = jnp.int32(0)
        for peer in circle:

            @pl.when(rank(peer["tp"]) > own_rank)
            def _(peer=peer):
                pl.semaphore_signal(barrier, inc=1, device_id=peer, device_id_type=MESH)

            above = above + jnp.where(rank(peer["tp"]) > own_rank, 1, 0)
        lower = lower + (len(circle) - above)
        higher.append(above)

    loads = []

    def load(src, dst):
        copy = pltpu.make_async_copy(src, dst, load_sem.at[len(loads)])
        copy.start()
        loads.append(copy)
        return copy

    first_loads = [load(tokens_in, tokens), load(gain_in, gain)]
    w_loads, mix_loads, mem_loads, cell_loads = [], [], [], []
    for b in range(blocks):
        w_loads.append(
            [load(w.at[b], wbuf.at[b, :, pl.ds(i * dk, dk)]) for i, w in enumerate((wq, wk, wv, wo))]
        )
        if b == 0:
            small = ((gate_in, gate_w), (bias_in, bias), (norm_in, norm), (stab_in, stab))
            cell_loads = [load(src, dst) for src, dst in small]
        mem_loads.append(load(memory.at[b, :, 0], membuf.at[b]))
        mix_loads.append(load(wmix.at[b], mixbuf.at[b]))

    def enter():
        with jax.named_scope("wait_barrier"):
            pl.semaphore_wait(barrier, lower)
        for i, circle in enumerate(circles):
            for peer in circle:

                @pl.when(rank(peer["tp"]) < own_rank)
                def _(peer=peer, i=i):
                    pl.semaphore_signal(token.at[i], inc=1, device_id=peer, device_id_type=MESH)

    def met(b, i):
        if b == 0:

            @pl.when(higher[i] > 0)
            def _():
                pl.semaphore_wait(token.at[i], higher[i])

    def rows_of(block):
        return pl.ds(pl.multiple_of(block * rows, rows), rows)

    sent = []

    def push(src, dst, send, recv, peer):
        copy = pltpu.make_async_remote_copy(
            src_ref=src, dst_ref=dst, send_sem=send, recv_sem=recv,
            device_id=peer, device_id_type=MESH,
        )
        copy.start()
        sent.append(copy)
        return copy

    for b in range(blocks):
        x_now = tokens if b == 0 else xbuf.at[b - 1]
        for copy in first_loads if b == 0 else ():
            copy.wait()
        xf = x_now[...].astype(jnp.float32)
        scaled_in = (xf * gain[b : b + 1, :]).astype(jnp.bfloat16)
        squares = jnp.sum(xf * xf, axis=-1, keepdims=True)
        high = squares.astype(jnp.bfloat16).astype(jnp.float32)
        lane = lax.broadcasted_iota(jnp.int32, (xf.shape[0], EXTRA), 1)
        tail = jnp.where(lane == 0, high, jnp.where(lane == 1, squares - high, 0.0))
        send1[b, :, cols:] = tail.astype(jnp.bfloat16)
        with jax.named_scope(f"wait_weights_{b}"):
            for copy in w_loads[b]:
                copy.wait()
        prod = jnp.dot(scaled_in, wbuf[b], preferred_element_type=jnp.float32)
        part[...] = prod
        send1[b, :, :cols] = prod.astype(jnp.bfloat16)
        if b == 0:
            enter()
        copies = [
            push(send1.at[b, rows_of(lax.rem(dp + k, n_dp))], recv1.at[b, k - 1],
                 s1.at[b, k - 1], r1.at[b, k - 1], at_dp(k))
            for k in ahead_first(n_dp)
        ]
        total = part[rows_of(dp), :]
        own_tail = send1[b, rows_of(dp), cols:].astype(jnp.float32)
        with jax.named_scope(f"wait_partials_{b}"):
            for copy in copies:
                copy.wait_recv()
        for k in range(1, n_dp):
            total = total + recv1[b, k - 1, :, :cols].astype(jnp.float32)
            own_tail = own_tail + recv1[b, k - 1, :, cols:].astype(jnp.float32)
        all_squares = jnp.sum(own_tail, axis=-1, keepdims=True)
        scale = lax.rsqrt(all_squares / model + EPS)
        proj = (scale * total).astype(jnp.bfloat16)
        query, key, value, outgate = (
            proj[:, i * dk : (i + 1) * dk].astype(jnp.float32) for i in range(4)
        )
        for copy in cell_loads if b == 0 else ():
            copy.wait()
        pre = lax.dot_general(
            proj[:, : 3 * dk], gate_w[b, 0], (((1,), (1,)), ((), ())), preferred_element_type=jnp.float32
        )
        log_input = pre[:, 0:1]
        shifted = pre[:, 1:2] + bias[:, b : b + 1]
        log_forget = jnp.minimum(shifted, 0.0) - jnp.log1p(jnp.exp(-jnp.abs(shifted)))
        old = jnp.sum(jnp.where(eye(rows), stab[b], 0.0), axis=1, keepdims=True)
        new_stab = jnp.maximum(log_forget + old, log_input)
        keep = jnp.exp(log_forget + old - new_stab)
        admit = jnp.exp(log_input - new_stab)
        scaled_key = key * dk ** (-0.5)
        admitted = admit * scaled_key
        new_norm = keep * norm[b, :, 0] + admitted
        mem_loads[b].wait()
        query_t = query.T
        recalled = jnp.concatenate(
            [
                jnp.sum(query_t[:, s : s + 1] * membuf[b, s], axis=0, keepdims=True)
                for s in range(rows)
            ],
            axis=0,
        )
        match = jnp.sum(query * admitted, axis=-1, keepdims=True)
        numer = keep * recalled + match * value
        denom = jnp.maximum(jnp.abs(jnp.sum(query * new_norm, axis=-1, keepdims=True)), 1.0)
        gated = numer / denom * jax.nn.sigmoid(outgate)
        gath[b, rows_of(dp), :] = gated.astype(jnp.bfloat16)
        copies = [
            push(gath.at[b, rows_of(dp)], gath.at[b, rows_of(dp)],
                 s2.at[b, k - 1], r2.at[b, k - 1], at_dp(k))
            for k in ahead_first(n_dp)
        ]
        vec_out[b, 0] = jnp.broadcast_to(keep, (rows, dk))
        vec_out[b, 1] = admitted
        vec_out[b, 2] = value
        vec_out[b, 3] = new_norm
        vec_out[b, 4] = jnp.broadcast_to(new_stab, (rows, dk))
        mix_loads[b].wait()
        with jax.named_scope(f"wait_gated_{b}"):
            for copy in copies:
                copy.wait_recv()
        prod = jnp.dot(gath[b], mixbuf[b], preferred_element_type=jnp.float32)
        mixpart[...] = prod
        send3[b] = prod.astype(jnp.bfloat16)
        met(b, 0)
        copies = [
            push(send3.at[b, rows_of(lax.rem(tp + k + n_tp, NEAR))], recv3.at[b, i],
                 s3.at[b, i], r3.at[b, i], at_tp(k))
            for i, k in enumerate(window)
        ]
        total = mixpart[rows_of(j), :]
        with jax.named_scope(f"wait_near_{b}"):
            for copy in copies:
                copy.wait_recv()
        for k in range(1, NEAR):
            total = total + recv3[b, k - 1].astype(jnp.float32)
        far[b, group] = total.astype(jnp.bfloat16)
        met(b, 1)
        copies = [
            push(far.at[b, group], far.at[b, group], s4.at[b, k - 1], r4.at[b, k - 1], at_tp(NEAR * k))
            for k in ahead_first(n_far)
        ]
        total = x_now[rows_of(j), :].astype(jnp.float32)
        with jax.named_scope(f"wait_far_{b}"):
            for copy in copies:
                copy.wait_recv()
        mixed = far[b, 0].astype(jnp.float32)
        for k in range(1, n_far):
            mixed = mixed + far[b, k].astype(jnp.float32)
        xbuf[b, rows_of(j), :] = (total + mixed).astype(jnp.bfloat16)
        copies = [
            push(xbuf.at[b, rows_of(j)], xbuf.at[b, rows_of(j)], s5.at[b, i], r5.at[b, i], at_tp(k))
            for i, k in enumerate(window)
        ]
        with jax.named_scope(f"wait_window_{b}"):
            for copy in copies:
                copy.wait_recv()
    x_out[...] = xbuf[blocks - 1]
    for copy in sent:
        copy.wait_send()


def finish_kernel(
    pieces, x_in, vec_in, memory_in, x_out, mem_out, norm_out, stab_out,
    x, vec, memory, fresh, new_norm, new_stab, load_sem, store_sem,
):
    blocks, rows, _, _ = memory.shape
    step = rows // pieces
    loads = [pltpu.make_async_copy(vec_in, vec, load_sem.at[0])]
    for b in range(blocks):
        for p in range(pieces):
            at = pl.ds(p * step, step)
            loads.append(
                pltpu.make_async_copy(memory_in.at[b, at, 0], memory.at[b, at], load_sem.at[len(loads)])
            )
    loads.append(pltpu.make_async_copy(x_in, x, load_sem.at[len(loads)]))
    for copy in loads:
        copy.start()
    stores = []

    def store(src, dst):
        copy = pltpu.make_async_copy(src, dst, store_sem.at[len(stores)])
        copy.start()
        stores.append(copy)

    loads[0].wait()
    for b in range(blocks):
        new_norm[b] = vec[b, 3]
        new_stab[b] = jnp.sum(jnp.where(eye(rows), vec[b, 4, :, :rows], 0.0), axis=0, keepdims=True)
        admitted_t = vec[b, 1].T
        for p in range(pieces):
            loads[1 + b * pieces + p].wait()
            for s in range(p * step, (p + 1) * step):
                fresh[b, s] = (
                    vec[b, 0, s : s + 1, :] * memory[b, s]
                    + admitted_t[:, s : s + 1] * vec[b, 2, s : s + 1, :]
                )
            at = pl.ds(p * step, step)
            store(fresh.at[b, at], mem_out.at[b, at, 0])
    loads[-1].wait()
    store(x, x_out)
    store(new_norm, norm_out.at[:, :, 0])
    store(new_stab, stab_out)
    for copy in stores:
        copy.wait()


def shards(n_dp, n_tp, *args):
    tokens, gain, wq, wk, wv, wo, gate_w, bias, wmix, memory, norm, stab = args
    blocks, rows, _, dk, _ = memory.shape
    seqs, feats = tokens.shape
    n_far = n_tp // NEAR
    dims = (blocks, rows, feats, dk, feats * n_dp)
    bf, f32 = jnp.bfloat16, jnp.float32
    gate_w, bias, stab = gate_w.transpose(0, 1, 3, 2), bias.T, stab.transpose(0, 2, 1)
    dma = pltpu.SemaphoreType.DMA
    x, vec = pl.pallas_call(
        functools.partial(step_kernel, n_dp, n_tp, dims),
        out_shape=(
            jax.ShapeDtypeStruct((seqs, feats), bf),
            jax.ShapeDtypeStruct((blocks, 5, rows, dk), f32),
        ),
        in_specs=[HBM] * 12,
        out_specs=(VM, VM),
        scratch_shapes=[
            *(pltpu.VMEM(a.shape, a.dtype) for a in (tokens, gain, gate_w, bias, norm, stab)),
            pltpu.VMEM((blocks, seqs, feats), bf),
            pltpu.VMEM((blocks, feats, 4 * dk), bf),
            pltpu.VMEM((blocks, dk, feats), bf),
            pltpu.VMEM((blocks, rows, dk, dk), f32),
            pltpu.VMEM((seqs, 4 * dk), f32),
            pltpu.VMEM((blocks, seqs, 4 * dk + EXTRA), bf),
            pltpu.VMEM((blocks, n_dp - 1, rows, 4 * dk + EXTRA), bf),
            pltpu.VMEM((blocks, seqs, dk), bf),
            pltpu.VMEM((seqs, feats), f32),
            pltpu.VMEM((blocks, seqs, feats), bf),
            pltpu.VMEM((blocks, NEAR - 1, rows, feats), bf),
            pltpu.VMEM((blocks, n_far, rows, feats), bf),
            dma((blocks * 6 + 6,)),
            pltpu.SemaphoreType.REGULAR((2,)),
            dma((blocks, n_dp - 1)),
            dma((blocks, n_dp - 1)),
            dma((blocks, n_dp - 1)),
            dma((blocks, n_dp - 1)),
            dma((blocks, NEAR - 1)),
            dma((blocks, NEAR - 1)),
            dma((blocks, n_far - 1)),
            dma((blocks, n_far - 1)),
            dma((blocks, NEAR - 1)),
            dma((blocks, NEAR - 1)),
        ],
        compiler_params=pltpu.CompilerParams(collective_id=0, has_side_effects=True),
        name="two_cells",
    )(tokens, gain, wq, wk, wv, wo, gate_w, bias, wmix, memory, norm, stab)
    pieces = 2
    copies = blocks * pieces
    x, new_memory, new_norm, new_stab = pl.pallas_call(
        functools.partial(finish_kernel, pieces),
        out_shape=(
            jax.ShapeDtypeStruct((seqs, feats), bf),
            jax.ShapeDtypeStruct(memory.shape, f32),
            jax.ShapeDtypeStruct(norm.shape, f32),
            jax.ShapeDtypeStruct(stab.shape, f32),
        ),
        in_specs=[HBM] * 3,
        out_specs=[HBM] * 4,
        scratch_shapes=[
            pltpu.VMEM((seqs, feats), bf),
            pltpu.VMEM((blocks, 5, rows, dk), f32),
            pltpu.VMEM((blocks, rows, dk, dk), f32),
            pltpu.VMEM((blocks, rows, dk, dk), f32),
            pltpu.VMEM((blocks, rows, dk), f32),
            pltpu.VMEM((blocks, 1, rows), f32),
            dma((copies + 2,)),
            dma((copies + 3,)),
        ],
        name="finish",
    )(x, vec, memory)
    return x, new_memory, new_norm, new_stab.transpose(0, 2, 1)


def solution(mesh):
    in_specs = (
        P("grp", "dp"),
        P(None, "dp"),
        P(None, "dp", "tp"),
        P(None, "dp", "tp"),
        P(None, "dp", "tp"),
        P(None, "dp", "tp"),
        P(None, "tp", None, None),
        P(None, "tp"),
        P(None, "tp", "dp"),
        P(None, ("grp", "dp"), "tp", None, None),
        P(None, ("grp", "dp"), "tp", None),
        P(None, ("grp", "dp"), "tp"),
    )
    out_specs = (
        P("grp", "dp"),
        P(None, ("grp", "dp"), "tp", None, None),
        P(None, ("grp", "dp"), "tp", None),
        P(None, ("grp", "dp"), "tp"),
    )
    body = functools.partial(shards, mesh.shape["dp"], mesh.shape["tp"])
    return jax.shard_map(body, mesh=mesh, in_specs=in_specs, out_specs=out_specs, check_vma=False)
```

```python
import functools

import jax
import jax.numpy as jnp
from jax import lax
from jax.experimental import pallas as pl
from jax.experimental.pallas import tpu as pltpu
from jax.sharding import PartitionSpec as P

EPS = 1e-06
MESH = pl.DeviceIdType.MESH
NEAR = 8
EXTRA = 128
HBM = pl.BlockSpec(memory_space=pltpu.HBM)
VM = pl.BlockSpec(memory_space=pltpu.VMEM)


def ahead_first(count):
    return sorted(range(1, count), key=lambda k: -min(k, count - k))


def eye(n):
    return lax.broadcasted_iota(jnp.int32, (n, n), 0) == lax.broadcasted_iota(jnp.int32, (n, n), 1)


def step_kernel(
    n_dp, n_tp, dims,
    tokens_in, gain_in, wq, wk, wv, wo, gate_in, bias_in, wmix, memory, norm_in, stab_in,
    x_out, vec_out,
    tokens, gain, gate_w, bias, norm, stab, vec, xbuf, wbuf, mixbuf, membuf, part, send1, recv1, gath, mixpart, send3, recv3, far,
    load_sem, store_sem, token, s1, r1, s2, r2, s3, r3, s4, r4, s5, r5,
):
    blocks, rows, feats, dk, model = dims
    cols = 4 * dk
    dp, tp = lax.axis_index("dp"), lax.axis_index("tp")
    n_far = n_tp // NEAR
    group, j = tp // NEAR, lax.rem(tp, NEAR)

    def at_dp(k):
        return {"dp": lax.rem(dp + k, n_dp)}

    def at_tp(k):
        return {"tp": lax.rem(tp + k + n_tp, n_tp)}

    window = sorted(range(-(NEAR // 2) + 1, NEAR // 2 + 1), key=lambda k: -abs(k))
    window = [k for k in window if k]

    loads = []

    def load(src, dst):
        copy = pltpu.make_async_copy(src, dst, load_sem.at[len(loads)])
        copy.start()
        loads.append(copy)
        return copy

    def load_weights(b):
        columns = (wbuf.at[b, :, pl.ds(i * dk, dk)] for i in range(4))
        return [load(w.at[b], dst) for w, dst in zip((wq, wk, wv, wo), columns)]

    first_loads = [load(tokens_in, tokens), load(gain_in, gain)]
    w_loads = [load_weights(0)]

    barrier = pltpu.get_barrier_semaphore()
    circles = [
        [at_tp(k) for h in range(NEAR // 2, 0, -1) for k in (h, -h)],
        [at_tp(NEAR * k) for k in ahead_first(n_far)],
    ]

    def rank(at):
        return jnp.where((at == 0) & (dp == 0), n_tp, at)

    own_rank = rank(tp)
    for k in ahead_first(n_dp):
        pl.semaphore_signal(barrier, inc=1, device_id=at_dp(k), device_id_type=MESH)
    lower, higher = jnp.int32(n_dp - 1), []
    for circle in circles:
        above = jnp.int32(0)
        for peer in circle:

            @pl.when(rank(peer["tp"]) > own_rank)
            def _(peer=peer):
                pl.semaphore_signal(barrier, inc=1, device_id=peer, device_id_type=MESH)

            above = above + jnp.where(rank(peer["tp"]) > own_rank, 1, 0)
        lower = lower + (len(circle) - above)
        higher.append(above)

    small = ((gate_in, gate_w), (bias_in, bias), (norm_in, norm), (stab_in, stab))
    cell_loads = [load(src, dst) for src, dst in small]
    mem_loads, mix_loads = [], []
    for b in range(blocks):
        if b:
            w_loads.append(load_weights(b))
        mem_loads.append(load(memory.at[b, :, 0], membuf.at[b]))
        mix_loads.append(load(wmix.at[b], mixbuf.at[b]))

    def enter():
        with jax.named_scope("wait_barrier"):
            pl.semaphore_wait(barrier, lower)
        for i, circle in enumerate(circles):
            for peer in circle:

                @pl.when(rank(peer["tp"]) < own_rank)
                def _(peer=peer, i=i):
                    pl.semaphore_signal(token.at[i], inc=1, device_id=peer, device_id_type=MESH)

    def met(b, i):
        if b == 0:

            @pl.when(higher[i] > 0)
            def _():
                pl.semaphore_wait(token.at[i], higher[i])

    def rows_of(block):
        return pl.ds(pl.multiple_of(block * rows, rows), rows)

    sent, stores = [], []

    def store(src, dst):
        copy = pltpu.make_async_copy(src, dst, store_sem.at[len(stores)])
        copy.start()
        stores.append(copy)

    def describe(src, dst, send, recv, peer):
        return pltpu.make_async_remote_copy(
            src_ref=src, dst_ref=dst, send_sem=send, recv_sem=recv,
            device_id=peer, device_id_type=MESH,
        )

    def push(*args):
        copy = describe(*args)
        copy.start()
        sent.append(copy)
        return copy

    for b in range(blocks):
        x_now = tokens if b == 0 else xbuf.at[b - 1]
        for copy in first_loads if b == 0 else ():
            copy.wait()
        xf = x_now[...].astype(jnp.float32)
        scaled_in = (xf * gain[b : b + 1, :]).astype(jnp.bfloat16)
        squares = jnp.sum(xf * xf, axis=-1, keepdims=True)
        high = squares.astype(jnp.bfloat16).astype(jnp.float32)
        lane = lax.broadcasted_iota(jnp.int32, (xf.shape[0], EXTRA), 1)
        tail = jnp.where(lane == 0, high, jnp.where(lane == 1, squares - high, 0.0))
        send1[b, :, cols:] = tail.astype(jnp.bfloat16)
        with jax.named_scope(f"wait_weights_{b}"):
            for copy in w_loads[b]:
                copy.wait()
        prod = jnp.dot(scaled_in, wbuf[b], preferred_element_type=jnp.float32)
        part[...] = prod
        send1[b, :, :cols] = prod.astype(jnp.bfloat16)
        if b == 0:
            enter()
        copies = [
            push(send1.at[b, rows_of(lax.rem(dp + k, n_dp))], recv1.at[b, k - 1],
                 s1.at[b, k - 1], r1.at[b, k - 1], at_dp(k))
            for k in ahead_first(n_dp)
        ]
        total = part[rows_of(dp), :]
        own_tail = send1[b, rows_of(dp), cols:].astype(jnp.float32)
        with jax.named_scope(f"wait_partials_{b}"):
            for copy in copies:
                copy.wait_recv()
        for k in range(1, n_dp):
            total = total + recv1[b, k - 1, :, :cols].astype(jnp.float32)
            own_tail = own_tail + recv1[b, k - 1, :, cols:].astype(jnp.float32)
        all_squares = jnp.sum(own_tail, axis=-1, keepdims=True)
        scale = lax.rsqrt(all_squares / model + EPS)
        proj = (scale * total).astype(jnp.bfloat16)
        query, key, value, outgate = (
            proj[:, i * dk : (i + 1) * dk].astype(jnp.float32) for i in range(4)
        )
        for copy in cell_loads if b == 0 else ():
            copy.wait()
        pre = lax.dot_general(
            proj[:, : 3 * dk], gate_w[b, 0], (((1,), (1,)), ((), ())), preferred_element_type=jnp.float32
        )
        log_input = pre[:, 0:1]
        shifted = pre[:, 1:2] + bias[:, b : b + 1]
        log_forget = jnp.minimum(shifted, 0.0) - jnp.log1p(jnp.exp(-jnp.abs(shifted)))
        old = jnp.sum(jnp.where(eye(rows), stab[b], 0.0), axis=1, keepdims=True)
        new_stab = jnp.maximum(log_forget + old, log_input)
        keep = jnp.exp(log_forget + old - new_stab)
        admit = jnp.exp(log_input - new_stab)
        scaled_key = key * dk ** (-0.5)
        admitted = admit * scaled_key
        new_norm = keep * norm[b, :, 0] + admitted
        mem_loads[b].wait()
        query_t = query.T
        recalled = jnp.concatenate(
            [
                jnp.sum(query_t[:, s : s + 1] * membuf[b, s], axis=0, keepdims=True)
                for s in range(rows)
            ],
            axis=0,
        )
        match = jnp.sum(query * admitted, axis=-1, keepdims=True)
        numer = keep * recalled + match * value
        denom = jnp.maximum(jnp.abs(jnp.sum(query * new_norm, axis=-1, keepdims=True)), 1.0)
        gated = numer / denom * jax.nn.sigmoid(outgate)
        gath[b, rows_of(dp), :] = gated.astype(jnp.bfloat16)
        copies = [
            push(gath.at[b, rows_of(dp)], gath.at[b, rows_of(dp)],
                 s2.at[b, k - 1], r2.at[b, k - 1], at_dp(k))
            for k in ahead_first(n_dp)
        ]
        vec[b, 0] = jnp.broadcast_to(keep, (rows, dk))
        vec[b, 1] = admitted
        vec[b, 2] = value
        vec[b, 3] = new_norm
        vec[b, 4] = jnp.broadcast_to(new_stab, (rows, dk))
        store(vec.at[b], vec_out.at[b])
        mix_loads[b].wait()
        with jax.named_scope(f"wait_gated_{b}"):
            for copy in copies:
                copy.wait_recv()
        prod = jnp.dot(gath[b], mixbuf[b], preferred_element_type=jnp.float32)
        mixpart[...] = prod
        send3[b] = prod.astype(jnp.bfloat16)
        met(b, 0)
        copies = [
            push(send3.at[b, rows_of(lax.rem(tp + k + n_tp, NEAR))], recv3.at[b, i],
                 s3.at[b, i], r3.at[b, i], at_tp(k))
            for i, k in enumerate(window)
        ]
        total = mixpart[rows_of(j), :]
        with jax.named_scope(f"wait_near_{b}"):
            for copy in copies:
                copy.wait_recv()
        for k in range(1, NEAR):
            total = total + recv3[b, k - 1].astype(jnp.float32)
        far[b, group] = total.astype(jnp.bfloat16)
        met(b, 1)
        last = b == blocks - 1
        copies, held = [], []
        for k in ahead_first(n_far):
            copy = describe(
                far.at[b, group], far.at[b, group], s4.at[b, k - 1], r4.at[b, k - 1], at_tp(NEAR * k)
            )
            copies.append(copy)
            to = lax.rem(group + k, n_far)
            inner = (group > 0) & (group < n_far - 1)
            now = inner | (to == 0) | (to == n_far - 1)
            if last:
                held.append((copy, now))
                pl.when(now)(copy.start)
            else:
                copy.start()
        sent += copies
        total = x_now[rows_of(j), :].astype(jnp.float32)
        with jax.named_scope(f"wait_far_{b}"):
            for copy in copies:
                copy.wait_recv()
        mixed = far[b, 0].astype(jnp.float32)
        for k in range(1, n_far):
            mixed = mixed + far[b, k].astype(jnp.float32)
        xbuf[b, rows_of(j), :] = (total + mixed).astype(jnp.bfloat16)
        x_next = x_out if last else xbuf.at[b]
        copies = [
            push(xbuf.at[b, rows_of(j)], x_next.at[rows_of(j)], s5.at[b, i], r5.at[b, i], at_tp(k))
            for i, k in enumerate(window)
        ]
        for copy, now in held:
            pl.when(jnp.logical_not(now))(copy.start)
        if last:
            store(xbuf.at[b, rows_of(j)], x_out.at[rows_of(j)])
        with jax.named_scope(f"wait_window_{b}"):
            for copy in copies:
                copy.wait_recv()
    for copy in sent:
        copy.wait_send()
    for copy in stores:
        copy.wait()


def finish_kernel(
    pieces, x_in, vec_in, memory_in, x_out, mem_out, norm_out, stab_out,
    x, vec, memory, fresh, new_norm, new_stab, load_sem, store_sem,
):
    blocks, rows, _, _ = memory.shape
    step = rows // pieces
    loads = [pltpu.make_async_copy(vec_in, vec, load_sem.at[0])]
    for b in range(blocks):
        for p in range(pieces):
            at = pl.ds(p * step, step)
            loads.append(
                pltpu.make_async_copy(memory_in.at[b, at, 0], memory.at[b, at], load_sem.at[len(loads)])
            )
    loads.append(pltpu.make_async_copy(x_in, x, load_sem.at[len(loads)]))
    for copy in loads:
        copy.start()
    stores = []

    def store(src, dst):
        copy = pltpu.make_async_copy(src, dst, store_sem.at[len(stores)])
        copy.start()
        stores.append(copy)

    loads[0].wait()
    for b in range(blocks):
        new_norm[b] = vec[b, 3]
        new_stab[b] = jnp.sum(jnp.where(eye(rows), vec[b, 4, :, :rows], 0.0), axis=0, keepdims=True)
        admitted_t = vec[b, 1].T
        for p in range(pieces):
            loads[1 + b * pieces + p].wait()
            for s in range(p * step, (p + 1) * step):
                fresh[b, s] = (
                    vec[b, 0, s : s + 1, :] * memory[b, s]
                    + admitted_t[:, s : s + 1] * vec[b, 2, s : s + 1, :]
                )
            at = pl.ds(p * step, step)
            store(fresh.at[b, at], mem_out.at[b, at, 0])
    loads[-1].wait()
    store(x, x_out)
    store(new_norm, norm_out.at[:, :, 0])
    store(new_stab, stab_out)
    for copy in stores:
        copy.wait()


def shards(n_dp, n_tp, *args):
    tokens, gain, wq, wk, wv, wo, gate_w, bias, wmix, memory, norm, stab = args
    blocks, rows, _, dk, _ = memory.shape
    seqs, feats = tokens.shape
    n_far = n_tp // NEAR
    dims = (blocks, rows, feats, dk, feats * n_dp)
    bf, f32 = jnp.bfloat16, jnp.float32
    gate_w, bias, stab = gate_w.transpose(0, 1, 3, 2), bias.T, stab.transpose(0, 2, 1)
    dma = pltpu.SemaphoreType.DMA
    x, vec = pl.pallas_call(
        functools.partial(step_kernel, n_dp, n_tp, dims),
        out_shape=(
            jax.ShapeDtypeStruct((seqs, feats), bf),
            jax.ShapeDtypeStruct((blocks, 5, rows, dk), f32),
        ),
        in_specs=[HBM] * 12,
        out_specs=(HBM, HBM),
        scratch_shapes=[
            *(pltpu.VMEM(a.shape, a.dtype) for a in (tokens, gain, gate_w, bias, norm, stab)),
            pltpu.VMEM((blocks, 5, rows, dk), f32),
            pltpu.VMEM((blocks, seqs, feats), bf),
            pltpu.VMEM((blocks, feats, 4 * dk), bf),
            pltpu.VMEM((blocks, dk, feats), bf),
            pltpu.VMEM((blocks, rows, dk, dk), f32),
            pltpu.VMEM((seqs, 4 * dk), f32),
            pltpu.VMEM((blocks, seqs, 4 * dk + EXTRA), bf),
            pltpu.VMEM((blocks, n_dp - 1, rows, 4 * dk + EXTRA), bf),
            pltpu.VMEM((blocks, seqs, dk), bf),
            pltpu.VMEM((seqs, feats), f32),
            pltpu.VMEM((blocks, seqs, feats), bf),
            pltpu.VMEM((blocks, NEAR - 1, rows, feats), bf),
            pltpu.VMEM((blocks, n_far, rows, feats), bf),
            dma((blocks * 6 + 6,)),
            dma((blocks + 1,)),
            pltpu.SemaphoreType.REGULAR((2,)),
            dma((blocks, n_dp - 1)),
            dma((blocks, n_dp - 1)),
            dma((blocks, n_dp - 1)),
            dma((blocks, n_dp - 1)),
            dma((blocks, NEAR - 1)),
            dma((blocks, NEAR - 1)),
            dma((blocks, n_far - 1)),
            dma((blocks, n_far - 1)),
            dma((blocks, NEAR - 1)),
            dma((blocks, NEAR - 1)),
        ],
        compiler_params=pltpu.CompilerParams(collective_id=0, has_side_effects=True),
        name="two_cells",
    )(tokens, gain, wq, wk, wv, wo, gate_w, bias, wmix, memory, norm, stab)
    pieces = 2
    copies = blocks * pieces
    x, new_memory, new_norm, new_stab = pl.pallas_call(
        functools.partial(finish_kernel, pieces),
        out_shape=(
            jax.ShapeDtypeStruct((seqs, feats), bf),
            jax.ShapeDtypeStruct(memory.shape, f32),
            jax.ShapeDtypeStruct(norm.shape, f32),
            jax.ShapeDtypeStruct(stab.shape, f32),
        ),
        in_specs=[HBM] * 3,
        out_specs=[HBM] * 4,
        scratch_shapes=[
            pltpu.VMEM((seqs, feats), bf),
            pltpu.VMEM((blocks, 5, rows, dk), f32),
            pltpu.VMEM((blocks, rows, dk, dk), f32),
            pltpu.VMEM((blocks, rows, dk, dk), f32),
            pltpu.VMEM((blocks, rows, dk), f32),
            pltpu.VMEM((blocks, 1, rows), f32),
            dma((copies + 2,)),
            dma((copies + 3,)),
        ],
        name="finish",
    )(x, vec, memory)
    return x, new_memory, new_norm, new_stab.transpose(0, 2, 1)


def solution(mesh):
    in_specs = (
        P("grp", "dp"),
        P(None, "dp"),
        P(None, "dp", "tp"),
        P(None, "dp", "tp"),
        P(None, "dp", "tp"),
        P(None, "dp", "tp"),
        P(None, "tp", None, None),
        P(None, "tp"),
        P(None, "tp", "dp"),
        P(None, ("grp", "dp"), "tp", None, None),
        P(None, ("grp", "dp"), "tp", None),
        P(None, ("grp", "dp"), "tp"),
    )
    out_specs = (
        P("grp", "dp"),
        P(None, ("grp", "dp"), "tp", None, None),
        P(None, ("grp", "dp"), "tp", None),
        P(None, ("grp", "dp"), "tp"),
    )
    body = functools.partial(shards, mesh.shape["dp"], mesh.shape["tp"])
    return jax.shard_map(body, mesh=mesh, in_specs=in_specs, out_specs=out_specs, check_vma=False)
```

```python
import functools

import jax
import jax.numpy as jnp
from jax import lax
from jax.experimental import pallas as pl
from jax.experimental.pallas import tpu as pltpu
from jax.sharding import PartitionSpec as P

EPS = 1e-06
MESH = pl.DeviceIdType.MESH
NEAR = 8
LANES = 128
HBM = pl.BlockSpec(memory_space=pltpu.HBM)
VM = pl.BlockSpec(memory_space=pltpu.VMEM)


def ahead_first(count):
    return sorted(range(1, count), key=lambda k: -min(k, count - k))


def eye(n, width=None):
    shape = (n, width or n)
    return lax.broadcasted_iota(jnp.int32, shape, 0) == lax.broadcasted_iota(jnp.int32, shape, 1)


def step_kernel(
    n_dp, n_tp, dims,
    tokens_in, gain_in, wq, wk, wv, wo, gate_in, bias_in, wmix, memory, norm_in, stab_in,
    x_out, vec_out,
    tokens, gain, gate_w, bias, norm, stab, vec, xbuf, wbuf, mixbuf, membuf, part, send1, recv1, gath, mixpart, send3, recv3, far,
    squares_out, squares_in, gmix, send6, recv6,
    load_sem, store_sem, token, s0, r0, s7, r7, s6, r6, s1, r1, s2, r2, s3, r3, s4, r4, s5, r5,
):
    blocks, rows, feats, dk, model = dims
    cols = 4 * dk
    dp, tp = lax.axis_index("dp"), lax.axis_index("tp")
    n_far = n_tp // NEAR
    group, j = tp // NEAR, lax.rem(tp, NEAR)

    def at_dp(k):
        return {"dp": lax.rem(dp + k, n_dp)}

    def at_tp(k):
        return {"tp": lax.rem(tp + k + n_tp, n_tp)}

    window = sorted(range(-(NEAR // 2) + 1, NEAR // 2 + 1), key=lambda k: -abs(k))
    window = [k for k in window if k]

    loads = []

    def load(src, dst):
        copy = pltpu.make_async_copy(src, dst, load_sem.at[len(loads)])
        copy.start()
        loads.append(copy)
        return copy

    def load_weights(b):
        columns = (wbuf.at[b, :, pl.ds(i * dk, dk)] for i in range(4))
        return [load(w.at[b], dst) for w, dst in zip((wq, wk, wv, wo), columns)]

    first_loads = [load(tokens_in, tokens), load(gain_in, gain)]
    w_loads = [load_weights(0)]

    barrier = pltpu.get_barrier_semaphore()
    circles = [
        [at_tp(k) for h in range(NEAR // 2, 0, -1) for k in (h, -h)],
        [at_tp(NEAR * k) for k in ahead_first(n_far)],
    ]

    def rank(at):
        return jnp.where((at == 0) & (dp == 0), n_tp, at)

    own_rank = rank(tp)
    for k in ahead_first(n_dp):
        pl.semaphore_signal(barrier, inc=1, device_id=at_dp(k), device_id_type=MESH)
    lower, higher = jnp.int32(n_dp - 1), []
    for circle in circles:
        above = jnp.int32(0)
        for peer in circle:

            @pl.when(rank(peer["tp"]) > own_rank)
            def _(peer=peer):
                pl.semaphore_signal(barrier, inc=1, device_id=peer, device_id_type=MESH)

            above = above + jnp.where(rank(peer["tp"]) > own_rank, 1, 0)
        lower = lower + (len(circle) - above)
        higher.append(above)

    small = ((gate_in, gate_w), (bias_in, bias), (norm_in, norm), (stab_in, stab))
    cell_loads = [load(src, dst) for src, dst in small]
    mem_loads, mix_loads = [], []
    for b in range(blocks):
        if b:
            w_loads.append(load_weights(b))
        mem_loads.append(load(memory.at[b, :, 0], membuf.at[b]))
        mix_loads.append(load(wmix.at[b], gmix.at[b, dp] if b else mixbuf))

    def enter():
        with jax.named_scope("wait_barrier"):
            pl.semaphore_wait(barrier, lower)
        for i, circle in enumerate(circles):
            for peer in circle:

                @pl.when(rank(peer["tp"]) < own_rank)
                def _(peer=peer, i=i):
                    pl.semaphore_signal(token.at[i], inc=1, device_id=peer, device_id_type=MESH)

    def met(b, i):
        if b == 0:

            @pl.when(higher[i] > 0)
            def _():
                pl.semaphore_wait(token.at[i], higher[i])

    def rows_of(block):
        return pl.ds(pl.multiple_of(block * rows, rows), rows)

    sent, stores = [], []

    def store(src, dst):
        copy = pltpu.make_async_copy(src, dst, store_sem.at[len(stores)])
        copy.start()
        stores.append(copy)

    def describe(src, dst, send, recv, peer):
        return pltpu.make_async_remote_copy(
            src_ref=src, dst_ref=dst, send_sem=send, recv_sem=recv,
            device_id=peer, device_id_type=MESH,
        )

    def push(*args):
        copy = describe(*args)
        copy.start()
        sent.append(copy)
        return copy

    for b in range(blocks):
        x_now = tokens if b == 0 else xbuf.at[b - 1]
        for copy in first_loads if b == 0 else ():
            copy.wait()
        xf = x_now[...].astype(jnp.float32)
        scaled_in = (xf * gain[b : b + 1, :]).astype(jnp.bfloat16)
        squares = jnp.sum(xf * xf, axis=-1, keepdims=True)
        spread = eye(rows, LANES)
        for k in range(n_dp):
            own = jnp.where(spread, squares[k * rows : (k + 1) * rows], 0.0)
            squares_out[b, k] = jnp.sum(own, axis=0, keepdims=True)
        with jax.named_scope(f"wait_weights_{b}"):
            for copy in w_loads[b]:
                copy.wait()
        prod = jnp.dot(scaled_in, wbuf[b], preferred_element_type=jnp.float32)
        part[...] = prod
        send1[b] = prod.astype(jnp.bfloat16)
        if b == 0:
            enter()
        copies = [
            push(send1.at[b, rows_of(lax.rem(dp + k, n_dp))], recv1.at[b, k - 1],
                 s1.at[b, k - 1], r1.at[b, k - 1], at_dp(k))
            for k in ahead_first(n_dp)
        ]
        copies += [
            push(squares_out.at[b, lax.rem(dp + k, n_dp)], squares_in.at[b, k - 1],
                 s0.at[b, k - 1], r0.at[b, k - 1], at_dp(k))
            for k in ahead_first(n_dp)
        ]
        total = part[rows_of(dp), :]
        all_squares = squares_out[b, dp]
        with jax.named_scope(f"wait_partials_{b}"):
            for copy in copies:
                copy.wait_recv()
        for k in range(1, n_dp):
            total = total + recv1[b, k - 1].astype(jnp.float32)
            all_squares = all_squares + squares_in[b, k - 1]
        all_squares = jnp.sum(jnp.where(spread, all_squares, 0.0), axis=1, keepdims=True)
        scale = lax.rsqrt(all_squares / model + EPS)
        proj = (scale * total).astype(jnp.bfloat16)
        query, key, value, outgate = (
            proj[:, i * dk : (i + 1) * dk].astype(jnp.float32) for i in range(4)
        )
        for copy in cell_loads if b == 0 else ():
            copy.wait()
        pre = lax.dot_general(
            proj[:, : 3 * dk], gate_w[b, 0], (((1,), (1,)), ((), ())), preferred_element_type=jnp.float32
        )
        log_input = pre[:, 0:1]
        shifted = pre[:, 1:2] + bias[:, b : b + 1]
        log_forget = jnp.minimum(shifted, 0.0) - jnp.log1p(jnp.exp(-jnp.abs(shifted)))
        old = jnp.sum(jnp.where(eye(rows), stab[b], 0.0), axis=1, keepdims=True)
        new_stab = jnp.maximum(log_forget + old, log_input)
        keep = jnp.exp(log_forget + old - new_stab)
        admit = jnp.exp(log_input - new_stab)
        scaled_key = key * dk ** (-0.5)
        admitted = admit * scaled_key
        new_norm = keep * norm[b, :, 0] + admitted
        mem_loads[b].wait()
        query_t = query.T
        recalled = jnp.concatenate(
            [
                jnp.sum(query_t[:, s : s + 1] * membuf[b, s], axis=0, keepdims=True)
                for s in range(rows)
            ],
            axis=0,
        )
        match = jnp.sum(query * admitted, axis=-1, keepdims=True)
        numer = keep * recalled + match * value
        denom = jnp.maximum(jnp.abs(jnp.sum(query * new_norm, axis=-1, keepdims=True)), 1.0)
        gated = numer / denom * jax.nn.sigmoid(outgate)
        gated = gated.astype(jnp.bfloat16)
        if b == 0:
            gath[rows_of(dp), :] = gated
            copies = [
                push(gath.at[rows_of(dp)], gath.at[rows_of(dp)], s2.at[k - 1], r2.at[k - 1], at_dp(k))
                for k in ahead_first(n_dp)
            ]
        else:
            for copy in mix_copies[b]:
                copy.wait_recv()
            turn = lax.rem(dp - tp + n_tp, NEAR)
            turn = jnp.where(turn > NEAR // 2, turn - NEAR, turn)
            slot = turn + NEAR // 2 - 1
            for k in range(n_dp):
                send6[b, k] = jnp.dot(
                    gated, gmix[b, k], preferred_element_type=jnp.float32
                ).astype(jnp.bfloat16)
            copies = []
            for k in ahead_first(n_dp):
                to = lax.rem(dp + k, n_dp)
                peer = {"dp": to, **at_tp(turn)}
                push(send6.at[b, to], recv6.at[b, slot], s6.at[b, k], r6.at[b, slot], peer)
            itself = describe(
                send6.at[b, dp], recv6.at[b, slot], s6.at[b, 0], r6.at[b, slot], at_tp(turn)
            )
            pl.when(turn != 0)(itself.start)

            @pl.when(turn == 0)
            def _():
                recv6[b, NEAR // 2 - 1] = send6[b, dp]
        vec[b, 0] = jnp.broadcast_to(keep, (rows, dk))
        vec[b, 1] = admitted
        vec[b, 2] = value
        vec[b, 3] = new_norm
        vec[b, 4] = jnp.broadcast_to(new_stab, (rows, dk))
        store(vec.at[b], vec_out.at[b])
        if b == 0:
            mix_loads[b].wait()
            with jax.named_scope(f"wait_gated_{b}"):
                for copy in copies:
                    copy.wait_recv()
            prod = jnp.dot(gath[...], mixbuf[...], preferred_element_type=jnp.float32)
            mixpart[...] = prod
            send3[...] = prod.astype(jnp.bfloat16)
            met(0, 0)
            copies = [
                push(send3.at[rows_of(lax.rem(tp + k + n_tp, NEAR))], recv3.at[i],
                     s3.at[i], r3.at[i], at_tp(k))
                for i, k in enumerate(window)
            ]
            mix_copies = {}
            for later in range(1, blocks):
                mix_loads[later].wait()
                mix_copies[later] = [
                    push(gmix.at[later, dp], gmix.at[later, dp],
                         s7.at[later, k - 1], r7.at[later, k - 1], at_dp(k))
                    for k in ahead_first(n_dp)
                ]
            total = mixpart[rows_of(j), :]
            with jax.named_scope(f"wait_near_{b}"):
                for copy in copies:
                    copy.wait_recv()
            for i in range(len(window)):
                total = total + recv3[i].astype(jnp.float32)
        else:
            with jax.named_scope(f"wait_near_{b}"):
                for i in range(NEAR):
                    arrived = describe(
                        send6.at[b, 0], recv6.at[b, i], s6.at[b, 0], r6.at[b, i], at_tp(turn)
                    )
                    if i == NEAR // 2 - 1:
                        pl.when(turn != 0)(arrived.wait_recv)
                    else:
                        arrived.wait_recv()
            total = sum(recv6[b, i].astype(jnp.float32) for i in range(NEAR))
        far[b, group] = total.astype(jnp.bfloat16)
        met(b, 1)
        copies = [
            push(far.at[b, group], far.at[b, group], s4.at[b, k - 1], r4.at[b, k - 1], at_tp(NEAR * k))
            for k in ahead_first(n_far)
        ]
        total = x_now[rows_of(j), :].astype(jnp.float32)
        with jax.named_scope(f"wait_far_{b}"):
            for copy in copies:
                copy.wait_recv()
        mixed = far[b, 0].astype(jnp.float32)
        for k in range(1, n_far):
            mixed = mixed + far[b, k].astype(jnp.float32)
        xbuf[b, rows_of(j), :] = (total + mixed).astype(jnp.bfloat16)
        last = b == blocks - 1
        x_next = x_out if last else xbuf.at[b]
        copies = [
            push(xbuf.at[b, rows_of(j)], x_next.at[rows_of(j)], s5.at[b, i], r5.at[b, i], at_tp(k))
            for i, k in enumerate(window)
        ]
        if last:
            store(xbuf.at[b, rows_of(j)], x_out.at[rows_of(j)])
        if last:
            for copy in sent[: -len(copies)]:
                copy.wait_send()
            pl.when(turn != 0)(itself.wait_send)
            for copy in stores[:-1]:
                copy.wait()
        with jax.named_scope(f"wait_window_{b}"):
            for copy in copies:
                copy.wait_recv()
    for copy in copies:
        copy.wait_send()
    stores[-1].wait()


def finish_kernel(
    pieces, x_in, vec_in, memory_in, x_out, mem_out, norm_out, stab_out,
    x, vec, memory, fresh, new_norm, new_stab, load_sem, store_sem,
):
    blocks, rows, _, _ = memory.shape
    step = rows // pieces
    loads = [pltpu.make_async_copy(vec_in, vec, load_sem.at[0])]
    for b in range(blocks):
        for p in range(pieces):
            at = pl.ds(p * step, step)
            loads.append(
                pltpu.make_async_copy(memory_in.at[b, at, 0], memory.at[b, at], load_sem.at[len(loads)])
            )
    loads.append(pltpu.make_async_copy(x_in, x, load_sem.at[len(loads)]))
    for copy in loads:
        copy.start()
    stores = []

    def store(src, dst):
        copy = pltpu.make_async_copy(src, dst, store_sem.at[len(stores)])
        copy.start()
        stores.append(copy)

    loads[0].wait()
    for b in range(blocks):
        new_norm[b] = vec[b, 3]
        new_stab[b] = jnp.sum(jnp.where(eye(rows), vec[b, 4, :, :rows], 0.0), axis=0, keepdims=True)
        admitted_t = vec[b, 1].T
        for p in range(pieces):
            loads[1 + b * pieces + p].wait()
            for s in range(p * step, (p + 1) * step):
                fresh[b, s] = (
                    vec[b, 0, s : s + 1, :] * memory[b, s]
                    + admitted_t[:, s : s + 1] * vec[b, 2, s : s + 1, :]
                )
            at = pl.ds(p * step, step)
            store(fresh.at[b, at], mem_out.at[b, at, 0])
    loads[-1].wait()
    store(x, x_out)
    store(new_norm, norm_out.at[:, :, 0])
    store(new_stab, stab_out)
    for copy in stores:
        copy.wait()


def shards(n_dp, n_tp, *args):
    tokens, gain, wq, wk, wv, wo, gate_w, bias, wmix, memory, norm, stab = args
    blocks, rows, _, dk, _ = memory.shape
    seqs, feats = tokens.shape
    n_far = n_tp // NEAR
    dims = (blocks, rows, feats, dk, feats * n_dp)
    bf, f32 = jnp.bfloat16, jnp.float32
    gate_w, bias, stab = gate_w.transpose(0, 1, 3, 2), bias.T, stab.transpose(0, 2, 1)
    dma = pltpu.SemaphoreType.DMA
    x, vec = pl.pallas_call(
        functools.partial(step_kernel, n_dp, n_tp, dims),
        out_shape=(
            jax.ShapeDtypeStruct((seqs, feats), bf),
            jax.ShapeDtypeStruct((blocks, 5, rows, dk), f32),
        ),
        in_specs=[HBM] * 12,
        out_specs=(HBM, HBM),
        scratch_shapes=[
            *(pltpu.VMEM(a.shape, a.dtype) for a in (tokens, gain, gate_w, bias, norm, stab)),
            pltpu.VMEM((blocks, 5, rows, dk), f32),
            pltpu.VMEM((blocks, seqs, feats), bf),
            pltpu.VMEM((blocks, feats, 4 * dk), bf),
            pltpu.VMEM((dk, feats), bf),
            pltpu.VMEM((blocks, rows, dk, dk), f32),
            pltpu.VMEM((seqs, 4 * dk), f32),
            pltpu.VMEM((blocks, seqs, 4 * dk), bf),
            pltpu.VMEM((blocks, n_dp - 1, rows, 4 * dk), bf),
            pltpu.VMEM((seqs, dk), bf),
            pltpu.VMEM((seqs, feats), f32),
            pltpu.VMEM((seqs, feats), bf),
            pltpu.VMEM((NEAR - 1, rows, feats), bf),
            pltpu.VMEM((blocks, n_far, rows, feats), bf),
            pltpu.VMEM((blocks, n_dp, 1, LANES), f32),
            pltpu.VMEM((blocks, n_dp - 1, 1, LANES), f32),
            pltpu.VMEM((blocks, n_dp, dk, feats), bf),
            pltpu.VMEM((blocks, n_dp, rows, feats), bf),
            pltpu.VMEM((blocks, NEAR, rows, feats), bf),
            dma((blocks * 6 + 6,)),
            dma((blocks + 1,)),
            pltpu.SemaphoreType.REGULAR((2,)),
            dma((blocks, n_dp - 1)),
            dma((blocks, n_dp - 1)),
            dma((blocks, n_dp - 1)),
            dma((blocks, n_dp - 1)),
            dma((blocks, n_dp)),
            dma((blocks, NEAR)),
            dma((blocks, n_dp - 1)),
            dma((blocks, n_dp - 1)),
            dma((n_dp - 1,)),
            dma((n_dp - 1,)),
            dma((NEAR - 1,)),
            dma((NEAR - 1,)),
            dma((blocks, n_far - 1)),
            dma((blocks, n_far - 1)),
            dma((blocks, NEAR - 1)),
            dma((blocks, NEAR - 1)),
        ],
        compiler_params=pltpu.CompilerParams(collective_id=0, has_side_effects=True),
        name="two_cells",
    )(tokens, gain, wq, wk, wv, wo, gate_w, bias, wmix, memory, norm, stab)
    pieces = 2
    copies = blocks * pieces
    x, new_memory, new_norm, new_stab = pl.pallas_call(
        functools.partial(finish_kernel, pieces),
        out_shape=(
            jax.ShapeDtypeStruct((seqs, feats), bf),
            jax.ShapeDtypeStruct(memory.shape, f32),
            jax.ShapeDtypeStruct(norm.shape, f32),
            jax.ShapeDtypeStruct(stab.shape, f32),
        ),
        in_specs=[HBM] * 3,
        out_specs=[HBM] * 4,
        scratch_shapes=[
            pltpu.VMEM((seqs, feats), bf),
            pltpu.VMEM((blocks, 5, rows, dk), f32),
            pltpu.VMEM((blocks, rows, dk, dk), f32),
            pltpu.VMEM((blocks, rows, dk, dk), f32),
            pltpu.VMEM((blocks, rows, dk), f32),
            pltpu.VMEM((blocks, 1, rows), f32),
            dma((copies + 2,)),
            dma((copies + 3,)),
        ],
        name="finish",
    )(x, vec, memory)
    return x, new_memory, new_norm, new_stab.transpose(0, 2, 1)


def solution(mesh):
    in_specs = (
        P("grp", "dp"),
        P(None, "dp"),
        P(None, "dp", "tp"),
        P(None, "dp", "tp"),
        P(None, "dp", "tp"),
        P(None, "dp", "tp"),
        P(None, "tp", None, None),
        P(None, "tp"),
        P(None, "tp", "dp"),
        P(None, ("grp", "dp"), "tp", None, None),
        P(None, ("grp", "dp"), "tp", None),
        P(None, ("grp", "dp"), "tp"),
    )
    out_specs = (
        P("grp", "dp"),
        P(None, ("grp", "dp"), "tp", None, None),
        P(None, ("grp", "dp"), "tp", None),
        P(None, ("grp", "dp"), "tp"),
    )
    body = functools.partial(shards, mesh.shape["dp"], mesh.shape["tp"])
    return jax.shard_map(body, mesh=mesh, in_specs=in_specs, out_specs=out_specs, check_vma=False)
```

```python
import functools

import jax
import jax.numpy as jnp
from jax import lax
from jax.experimental import pallas as pl
from jax.experimental.pallas import tpu as pltpu
from jax.sharding import PartitionSpec as P

EPS = 1e-06
MESH = pl.DeviceIdType.MESH
NEAR = 8
LANES = 128
HBM = pl.BlockSpec(memory_space=pltpu.HBM)
VM = pl.BlockSpec(memory_space=pltpu.VMEM)


def ahead_first(count):
    return sorted(range(1, count), key=lambda k: -min(k, count - k))


def eye(n, width=None):
    shape = (n, width or n)
    return lax.broadcasted_iota(jnp.int32, shape, 0) == lax.broadcasted_iota(jnp.int32, shape, 1)


def step_kernel(
    n_dp, n_tp, dims,
    tokens_in, gain_in, wq, wk, wv, wo, gate_in, bias_in, wmix, memory, norm_in, stab_in,
    x_out, vec_out,
    tokens, gain, gate_w, bias, norm, stab, vec, xbuf, wbuf, mixbuf, membuf, part, send1, recv1, gath, mixpart, send3, recv3, far,
    squares_out, squares_in, gmix, send6, recv6,
    load_sem, store_sem, token, s0, r0, s7, r7, s6, r6, s1, r1, s2, r2, s3, r3, s4, r4, s5, r5,
):
    blocks, rows, feats, dk, model = dims
    cols = 4 * dk
    dp, tp = lax.axis_index("dp"), lax.axis_index("tp")
    n_far = n_tp // NEAR
    group, j = tp // NEAR, lax.rem(tp, NEAR)

    def at_dp(k):
        return {"dp": lax.rem(dp + k, n_dp)}

    def at_tp(k):
        return {"tp": lax.rem(tp + k + n_tp, n_tp)}

    window = sorted(range(-(NEAR // 2) + 1, NEAR // 2 + 1), key=lambda k: -abs(k))
    window = [k for k in window if k]

    loads = []

    def load(src, dst):
        copy = pltpu.make_async_copy(src, dst, load_sem.at[len(loads)])
        copy.start()
        loads.append(copy)
        return copy

    def load_weights(b):
        columns = (wbuf.at[b, :, pl.ds(i * dk, dk)] for i in range(4))
        return [load(w.at[b], dst) for w, dst in zip((wq, wk, wv, wo), columns)]

    first_loads = [load(tokens_in, tokens), load(gain_in, gain)]
    w_loads = [load_weights(0)]

    barrier = pltpu.get_barrier_semaphore()
    circles = [
        [at_tp(k) for h in range(NEAR // 2, 0, -1) for k in (h, -h)],
        [at_tp(NEAR * k) for k in ahead_first(n_far)],
    ]

    def rank(at):
        return jnp.where((at == 0) & (dp == 0), n_tp, at)

    own_rank = rank(tp)
    for k in ahead_first(n_dp):
        pl.semaphore_signal(barrier, inc=1, device_id=at_dp(k), device_id_type=MESH)
    lower, higher = jnp.int32(n_dp - 1), []
    for circle in circles:
        above = jnp.int32(0)
        for peer in circle:

            @pl.when(rank(peer["tp"]) > own_rank)
            def _(peer=peer):
                pl.semaphore_signal(barrier, inc=1, device_id=peer, device_id_type=MESH)

            above = above + jnp.where(rank(peer["tp"]) > own_rank, 1, 0)
        lower = lower + (len(circle) - above)
        higher.append(above)

    small = ((gate_in, gate_w), (bias_in, bias), (norm_in, norm), (stab_in, stab))
    cell_loads = [load(src, dst) for src, dst in small]
    mem_loads, mix_loads = [], []
    for b in range(blocks):
        if b:
            w_loads.append(load_weights(b))
        mem_loads.append(load(memory.at[b, :, 0], membuf.at[b]))
        mix_loads.append(load(wmix.at[b], gmix.at[b, dp] if b else mixbuf))

    def enter():
        with jax.named_scope("wait_barrier"):
            pl.semaphore_wait(barrier, lower)
        for i, circle in enumerate(circles):
            for peer in circle:

                @pl.when(rank(peer["tp"]) < own_rank)
                def _(peer=peer, i=i):
                    pl.semaphore_signal(token.at[i], inc=1, device_id=peer, device_id_type=MESH)

    def met(b, i):
        if b == 0:

            @pl.when(higher[i] > 0)
            def _():
                pl.semaphore_wait(token.at[i], higher[i])

    def rows_of(block):
        return pl.ds(pl.multiple_of(block * rows, rows), rows)

    sent, stores = [], []

    def store(src, dst):
        copy = pltpu.make_async_copy(src, dst, store_sem.at[len(stores)])
        copy.start()
        stores.append(copy)

    def describe(src, dst, send, recv, peer):
        return pltpu.make_async_remote_copy(
            src_ref=src, dst_ref=dst, send_sem=send, recv_sem=recv,
            device_id=peer, device_id_type=MESH,
        )

    def push(*args):
        copy = describe(*args)
        copy.start()
        sent.append(copy)
        return copy

    for b in range(blocks):
        x_now = tokens if b == 0 else xbuf.at[b - 1]
        for copy in first_loads if b == 0 else ():
            copy.wait()
        xf = x_now[...].astype(jnp.float32)
        scaled_in = (xf * gain[b : b + 1, :]).astype(jnp.bfloat16)
        squares = jnp.sum(xf * xf, axis=-1, keepdims=True)
        spread = eye(rows, LANES)
        for k in range(n_dp):
            own = jnp.where(spread, squares[k * rows : (k + 1) * rows], 0.0)
            squares_out[b, k] = jnp.sum(own, axis=0, keepdims=True)
        with jax.named_scope(f"wait_weights_{b}"):
            for copy in w_loads[b]:
                copy.wait()
        prod = jnp.dot(scaled_in, wbuf[b], preferred_element_type=jnp.float32)
        part[...] = prod
        send1[b] = prod.astype(jnp.bfloat16)
        if b == 0:
            enter()
        copies = [
            push(send1.at[b, rows_of(lax.rem(dp + k, n_dp))], recv1.at[b, k - 1],
                 s1.at[b, k - 1], r1.at[b, k - 1], at_dp(k))
            for k in ahead_first(n_dp)
        ]
        copies += [
            push(squares_out.at[b, lax.rem(dp + k, n_dp)], squares_in.at[b, k - 1],
                 s0.at[b, k - 1], r0.at[b, k - 1], at_dp(k))
            for k in ahead_first(n_dp)
        ]
        total = part[rows_of(dp), :]
        all_squares = squares_out[b, dp]
        with jax.named_scope(f"wait_partials_{b}"):
            for copy in copies:
                copy.wait_recv()
        for k in range(1, n_dp):
            total = total + recv1[b, k - 1].astype(jnp.float32)
            all_squares = all_squares + squares_in[b, k - 1]
        all_squares = jnp.sum(jnp.where(spread, all_squares, 0.0), axis=1, keepdims=True)
        scale = lax.rsqrt(all_squares / model + EPS)
        proj = (scale * total).astype(jnp.bfloat16)
        query, key, value, outgate = (
            proj[:, i * dk : (i + 1) * dk].astype(jnp.float32) for i in range(4)
        )
        for copy in cell_loads if b == 0 else ():
            copy.wait()
        pre = lax.dot_general(
            proj[:, : 3 * dk], gate_w[b, 0], (((1,), (1,)), ((), ())), preferred_element_type=jnp.float32
        )
        log_input = pre[:, 0:1]
        shifted = pre[:, 1:2] + bias[:, b : b + 1]
        log_forget = jnp.minimum(shifted, 0.0) - jnp.log1p(jnp.exp(-jnp.abs(shifted)))
        old = jnp.sum(jnp.where(eye(rows), stab[b], 0.0), axis=1, keepdims=True)
        new_stab = jnp.maximum(log_forget + old, log_input)
        keep = jnp.exp(log_forget + old - new_stab)
        admit = jnp.exp(log_input - new_stab)
        scaled_key = key * dk ** (-0.5)
        admitted = admit * scaled_key
        new_norm = keep * norm[b, :, 0] + admitted
        mem_loads[b].wait()
        query_t = query.T
        recalled = jnp.concatenate(
            [
                jnp.sum(query_t[:, s : s + 1] * membuf[b, s], axis=0, keepdims=True)
                for s in range(rows)
            ],
            axis=0,
        )
        match = jnp.sum(query * admitted, axis=-1, keepdims=True)
        numer = keep * recalled + match * value
        denom = jnp.maximum(jnp.abs(jnp.sum(query * new_norm, axis=-1, keepdims=True)), 1.0)
        gated = numer / denom * jax.nn.sigmoid(outgate)
        gated = gated.astype(jnp.bfloat16)
        if b == 0:
            own_block = j
            gath[rows_of(dp), :] = gated
            copies = [
                push(gath.at[rows_of(dp)], gath.at[rows_of(dp)], s2.at[k - 1], r2.at[k - 1], at_dp(k))
                for k in ahead_first(n_dp)
            ]
        else:
            for copy in mix_copies[b]:
                copy.wait_recv()
            for k in range(n_dp):
                send6[b, k] = jnp.dot(
                    gated, gmix[b, k], preferred_element_type=jnp.float32
                ).astype(jnp.bfloat16)
            copies = []
            for k in (*ahead_first(n_dp), 0):
                to = lax.rem(dp + k, n_dp)
                turn = lax.rem(dp + to - tp + n_tp, NEAR)
                turn = jnp.where(turn > NEAR // 2, turn - NEAR, turn)
                slot = turn + NEAR // 2 - 1
                copy = describe(
                    send6.at[b, to], recv6.at[b, slot], s6.at[b, k], r6.at[b, slot],
                    {"dp": to, **at_tp(turn)},
                )
                if k:
                    copy.start()
                    sent.append(copy)
            pl.when(turn != 0)(copy.start)
            itself = copy

            @pl.when(turn == 0)
            def _():
                recv6[b, NEAR // 2 - 1] = send6[b, dp]
            own_block = lax.rem(tp - dp + n_dp, NEAR)
        vec[b, 0] = jnp.broadcast_to(keep, (rows, dk))
        vec[b, 1] = admitted
        vec[b, 2] = value
        vec[b, 3] = new_norm
        vec[b, 4] = jnp.broadcast_to(new_stab, (rows, dk))
        store(vec.at[b], vec_out.at[b])
        if b == 0:
            mix_loads[b].wait()
            with jax.named_scope(f"wait_gated_{b}"):
                for copy in copies:
                    copy.wait_recv()
            prod = jnp.dot(gath[...], mixbuf[...], preferred_element_type=jnp.float32)
            mixpart[...] = prod
            send3[...] = prod.astype(jnp.bfloat16)
            met(0, 0)
            copies = [
                push(send3.at[rows_of(lax.rem(tp + k + n_tp, NEAR))], recv3.at[i],
                     s3.at[i], r3.at[i], at_tp(k))
                for i, k in enumerate(window)
            ]
            mix_copies = {}
            for later in range(1, blocks):
                mix_loads[later].wait()
                mix_copies[later] = [
                    push(gmix.at[later, dp], gmix.at[later, dp],
                         s7.at[later, k - 1], r7.at[later, k - 1], at_dp(k))
                    for k in ahead_first(n_dp)
                ]
            total = mixpart[rows_of(j), :]
            with jax.named_scope(f"wait_near_{b}"):
                for copy in copies:
                    copy.wait_recv()
            for i in range(len(window)):
                total = total + recv3[i].astype(jnp.float32)
        else:
            with jax.named_scope(f"wait_near_{b}"):
                for i in range(NEAR):
                    arrived = describe(
                        send6.at[b, 0], recv6.at[b, i], s6.at[b, 0], r6.at[b, i], at_tp(turn)
                    )
                    if i == NEAR // 2 - 1:
                        pl.when(turn != 0)(arrived.wait_recv)
                    else:
                        arrived.wait_recv()
            total = sum(recv6[b, i].astype(jnp.float32) for i in range(NEAR))
        far[b, group] = total.astype(jnp.bfloat16)
        met(b, 1)
        copies = [
            push(far.at[b, group], far.at[b, group], s4.at[b, k - 1], r4.at[b, k - 1], at_tp(NEAR * k))
            for k in ahead_first(n_far)
        ]
        total = x_now[rows_of(own_block), :].astype(jnp.float32)
        with jax.named_scope(f"wait_far_{b}"):
            for copy in copies:
                copy.wait_recv()
        mixed = far[b, 0].astype(jnp.float32)
        for k in range(1, n_far):
            mixed = mixed + far[b, k].astype(jnp.float32)
        xbuf[b, rows_of(own_block), :] = (total + mixed).astype(jnp.bfloat16)
        last = b == blocks - 1
        x_next = x_out if last else xbuf.at[b]
        copies = [
            push(xbuf.at[b, rows_of(own_block)], x_next.at[rows_of(own_block)], s5.at[b, i], r5.at[b, i], at_tp(k))
            for i, k in enumerate(window)
        ]
        if last:
            store(xbuf.at[b, rows_of(own_block)], x_out.at[rows_of(own_block)])
        if last:
            for copy in sent[: -len(copies)]:
                copy.wait_send()
            pl.when(turn != 0)(itself.wait_send)
            for copy in stores[:-1]:
                copy.wait()
        with jax.named_scope(f"wait_window_{b}"):
            for copy in copies:
                copy.wait_recv()
    for copy in copies:
        copy.wait_send()
    stores[-1].wait()


def finish_kernel(
    pieces, x_in, vec_in, memory_in, x_out, mem_out, norm_out, stab_out,
    x, vec, memory, fresh, new_norm, new_stab, load_sem, store_sem,
):
    blocks, rows, _, _ = memory.shape
    step = rows // pieces
    loads = [pltpu.make_async_copy(vec_in, vec, load_sem.at[0])]
    for b in range(blocks):
        for p in range(pieces):
            at = pl.ds(p * step, step)
            loads.append(
                pltpu.make_async_copy(memory_in.at[b, at, 0], memory.at[b, at], load_sem.at[len(loads)])
            )
    loads.append(pltpu.make_async_copy(x_in, x, load_sem.at[len(loads)]))
    for copy in loads:
        copy.start()
    stores = []

    def store(src, dst):
        copy = pltpu.make_async_copy(src, dst, store_sem.at[len(stores)])
        copy.start()
        stores.append(copy)

    loads[0].wait()
    for b in range(blocks):
        new_norm[b] = vec[b, 3]
        new_stab[b] = jnp.sum(jnp.where(eye(rows), vec[b, 4, :, :rows], 0.0), axis=0, keepdims=True)
        admitted_t = vec[b, 1].T
        for p in range(pieces):
            loads[1 + b * pieces + p].wait()
            for s in range(p * step, (p + 1) * step):
                fresh[b, s] = (
                    vec[b, 0, s : s + 1, :] * memory[b, s]
                    + admitted_t[:, s : s + 1] * vec[b, 2, s : s + 1, :]
                )
            at = pl.ds(p * step, step)
            store(fresh.at[b, at], mem_out.at[b, at, 0])
    loads[-1].wait()
    store(x, x_out)
    store(new_norm, norm_out.at[:, :, 0])
    store(new_stab, stab_out)
    for copy in stores:
        copy.wait()


def shards(n_dp, n_tp, *args):
    tokens, gain, wq, wk, wv, wo, gate_w, bias, wmix, memory, norm, stab = args
    blocks, rows, _, dk, _ = memory.shape
    seqs, feats = tokens.shape
    n_far = n_tp // NEAR
    dims = (blocks, rows, feats, dk, feats * n_dp)
    bf, f32 = jnp.bfloat16, jnp.float32
    gate_w, bias, stab = gate_w.transpose(0, 1, 3, 2), bias.T, stab.transpose(0, 2, 1)
    dma = pltpu.SemaphoreType.DMA
    x, vec = pl.pallas_call(
        functools.partial(step_kernel, n_dp, n_tp, dims),
        out_shape=(
            jax.ShapeDtypeStruct((seqs, feats), bf),
            jax.ShapeDtypeStruct((blocks, 5, rows, dk), f32),
        ),
        in_specs=[HBM] * 12,
        out_specs=(HBM, HBM),
        scratch_shapes=[
            *(pltpu.VMEM(a.shape, a.dtype) for a in (tokens, gain, gate_w, bias, norm, stab)),
            pltpu.VMEM((blocks, 5, rows, dk), f32),
            pltpu.VMEM((blocks, seqs, feats), bf),
            pltpu.VMEM((blocks, feats, 4 * dk), bf),
            pltpu.VMEM((dk, feats), bf),
            pltpu.VMEM((blocks, rows, dk, dk), f32),
            pltpu.VMEM((seqs, 4 * dk), f32),
            pltpu.VMEM((blocks, seqs, 4 * dk), bf),
            pltpu.VMEM((blocks, n_dp - 1, rows, 4 * dk), bf),
            pltpu.VMEM((seqs, dk), bf),
            pltpu.VMEM((seqs, feats), f32),
            pltpu.VMEM((seqs, feats), bf),
            pltpu.VMEM((NEAR - 1, rows, feats), bf),
            pltpu.VMEM((blocks, n_far, rows, feats), bf),
            pltpu.VMEM((blocks, n_dp, 1, LANES), f32),
            pltpu.VMEM((blocks, n_dp - 1, 1, LANES), f32),
            pltpu.VMEM((blocks, n_dp, dk, feats), bf),
            pltpu.VMEM((blocks, n_dp, rows, feats), bf),
            pltpu.VMEM((blocks, NEAR, rows, feats), bf),
            dma((blocks * 6 + 6,)),
            dma((blocks + 1,)),
            pltpu.SemaphoreType.REGULAR((2,)),
            dma((blocks, n_dp - 1)),
            dma((blocks, n_dp - 1)),
            dma((blocks, n_dp - 1)),
            dma((blocks, n_dp - 1)),
            dma((blocks, n_dp)),
            dma((blocks, NEAR)),
            dma((blocks, n_dp - 1)),
            dma((blocks, n_dp - 1)),
            dma((n_dp - 1,)),
            dma((n_dp - 1,)),
            dma((NEAR - 1,)),
            dma((NEAR - 1,)),
            dma((blocks, n_far - 1)),
            dma((blocks, n_far - 1)),
            dma((blocks, NEAR - 1)),
            dma((blocks, NEAR - 1)),
        ],
        compiler_params=pltpu.CompilerParams(collective_id=0, has_side_effects=True),
        name="two_cells",
    )(tokens, gain, wq, wk, wv, wo, gate_w, bias, wmix, memory, norm, stab)
    pieces = 2
    copies = blocks * pieces
    x, new_memory, new_norm, new_stab = pl.pallas_call(
        functools.partial(finish_kernel, pieces),
        out_shape=(
            jax.ShapeDtypeStruct((seqs, feats), bf),
            jax.ShapeDtypeStruct(memory.shape, f32),
            jax.ShapeDtypeStruct(norm.shape, f32),
            jax.ShapeDtypeStruct(stab.shape, f32),
        ),
        in_specs=[HBM] * 3,
        out_specs=[HBM] * 4,
        scratch_shapes=[
            pltpu.VMEM((seqs, feats), bf),
            pltpu.VMEM((blocks, 5, rows, dk), f32),
            pltpu.VMEM((blocks, rows, dk, dk), f32),
            pltpu.VMEM((blocks, rows, dk, dk), f32),
            pltpu.VMEM((blocks, rows, dk), f32),
            pltpu.VMEM((blocks, 1, rows), f32),
            dma((copies + 2,)),
            dma((copies + 3,)),
        ],
        name="finish",
    )(x, vec, memory)
    return x, new_memory, new_norm, new_stab.transpose(0, 2, 1)


def solution(mesh):
    in_specs = (
        P("grp", "dp"),
        P(None, "dp"),
        P(None, "dp", "tp"),
        P(None, "dp", "tp"),
        P(None, "dp", "tp"),
        P(None, "dp", "tp"),
        P(None, "tp", None, None),
        P(None, "tp"),
        P(None, "tp", "dp"),
        P(None, ("grp", "dp"), "tp", None, None),
        P(None, ("grp", "dp"), "tp", None),
        P(None, ("grp", "dp"), "tp"),
    )
    out_specs = (
        P("grp", "dp"),
        P(None, ("grp", "dp"), "tp", None, None),
        P(None, ("grp", "dp"), "tp", None),
        P(None, ("grp", "dp"), "tp"),
    )
    body = functools.partial(shards, mesh.shape["dp"], mesh.shape["tp"])
    return jax.shard_map(body, mesh=mesh, in_specs=in_specs, out_specs=out_specs, check_vma=False)
```

```python
import functools

import jax
import jax.numpy as jnp
from jax import lax
from jax.experimental import pallas as pl
from jax.experimental.pallas import tpu as pltpu
from jax.sharding import PartitionSpec as P

EPS = 1e-06
MESH = pl.DeviceIdType.MESH
NEAR = 8
LANES = 128
HBM = pl.BlockSpec(memory_space=pltpu.HBM)
VM = pl.BlockSpec(memory_space=pltpu.VMEM)


def ahead_first(count):
    return sorted(range(1, count), key=lambda k: -min(k, count - k))


def eye(n, width=None):
    shape = (n, width or n)
    return lax.broadcasted_iota(jnp.int32, shape, 0) == lax.broadcasted_iota(jnp.int32, shape, 1)


def step_kernel(
    n_dp, n_tp, dims,
    tokens_in, gain_in, wq, wk, wv, wo, gate_in, bias_in, wmix, memory, norm_in, stab_in,
    x_out, vec_out,
    tokens, gain, gate_w, bias, norm, stab, vec, xbuf, wbuf, mixbuf, membuf, part, send1, recv1, gath, mixpart, send3, recv3, far,
    squares_out, squares_in, gmix, send6, recv6,
    load_sem, w_sem, store_sem, token, s0, r0, s7, r7, s6, r6, s1, r1, s2, r2, s3, r3, s4, r4, s5, r5,
):
    blocks, rows, feats, dk, model = dims
    cols = 4 * dk
    dp, tp = lax.axis_index("dp"), lax.axis_index("tp")
    n_far = n_tp // NEAR
    group, j = tp // NEAR, lax.rem(tp, NEAR)

    def at_dp(k):
        return {"dp": lax.rem(dp + k, n_dp)}

    def at_tp(k):
        return {"tp": lax.rem(tp + k + n_tp, n_tp)}

    window = sorted(range(-(NEAR // 2) + 1, NEAR // 2 + 1), key=lambda k: -abs(k))
    window = [k for k in window if k]

    loads = []

    def load(src, dst):
        copy = pltpu.make_async_copy(src, dst, load_sem.at[len(loads)])
        copy.start()
        loads.append(copy)
        return copy

    def load_weights(b):
        for i, w in enumerate((wq, wk, wv, wo)):
            pltpu.make_async_copy(w.at[b], wbuf.at[b, :, pl.ds(i * dk, dk)], w_sem.at[b]).start()
        return pltpu.make_async_copy(wbuf.at[b], wbuf.at[b], w_sem.at[b])

    first_loads = [load(tokens_in, tokens), load(gain_in, gain)]
    w_loads = [load_weights(0)]

    barrier = pltpu.get_barrier_semaphore()
    circles = [
        [at_tp(k) for h in range(NEAR // 2, 0, -1) for k in (h, -h)],
        [at_tp(NEAR * k) for k in ahead_first(n_far)],
    ]

    def rank(at):
        return jnp.where((at == 0) & (dp == 0), n_tp, at)

    own_rank = rank(tp)
    for k in ahead_first(n_dp):
        pl.semaphore_signal(barrier, inc=1, device_id=at_dp(k), device_id_type=MESH)
    lower, higher = jnp.int32(n_dp - 1), []
    for circle in circles:
        above = jnp.int32(0)
        for peer in circle:

            @pl.when(rank(peer["tp"]) > own_rank)
            def _(peer=peer):
                pl.semaphore_signal(barrier, inc=1, device_id=peer, device_id_type=MESH)

            above = above + jnp.where(rank(peer["tp"]) > own_rank, 1, 0)
        lower = lower + (len(circle) - above)
        higher.append(above)

    small = ((gate_in, gate_w), (bias_in, bias), (norm_in, norm), (stab_in, stab))
    cell_loads = [load(src, dst) for src, dst in small]
    mem_loads, mix_loads = [], []
    for b in range(blocks):
        if b:
            w_loads.append(load_weights(b))
        mem_loads.append(load(memory.at[b, :, 0], membuf.at[b]))
        mix_loads.append(load(wmix.at[b], gmix.at[b, dp] if b else mixbuf))

    def enter():
        with jax.named_scope("wait_barrier"):
            pl.semaphore_wait(barrier, lower)
        for i, circle in enumerate(circles):
            for peer in circle:

                @pl.when(rank(peer["tp"]) < own_rank)
                def _(peer=peer, i=i):
                    pl.semaphore_signal(token.at[i], inc=1, device_id=peer, device_id_type=MESH)

    def met(b, i):
        if b == 0:

            @pl.when(higher[i] > 0)
            def _():
                pl.semaphore_wait(token.at[i], higher[i])

    def rows_of(block):
        return pl.ds(pl.multiple_of(block * rows, rows), rows)

    sent, stores = [], []

    def store(src, dst):
        copy = pltpu.make_async_copy(src, dst, store_sem.at[len(stores)])
        copy.start()
        stores.append(copy)

    def describe(src, dst, send, recv, peer):
        return pltpu.make_async_remote_copy(
            src_ref=src, dst_ref=dst, send_sem=send, recv_sem=recv,
            device_id=peer, device_id_type=MESH,
        )

    def push(*args):
        describe(*args).start()

    def all_of(ref, send, recv):
        copy = describe(ref, ref, send, recv, at_dp(1))
        sent.append(copy)
        return copy

    for b in range(blocks):
        x_now = tokens if b == 0 else xbuf.at[b - 1]
        for copy in first_loads if b == 0 else ():
            copy.wait()
        xf = x_now[...].astype(jnp.float32)
        scaled_in = (xf * gain[b : b + 1, :]).astype(jnp.bfloat16)
        squares = jnp.sum(xf * xf, axis=-1, keepdims=True)
        spread = eye(rows, LANES)
        for k in range(n_dp):
            own = jnp.where(spread, squares[k * rows : (k + 1) * rows], 0.0)
            squares_out[b, k] = jnp.sum(own, axis=0, keepdims=True)
        with jax.named_scope(f"wait_weights_{b}"):
            w_loads[b].wait()
        prod = jnp.dot(scaled_in, wbuf[b], preferred_element_type=jnp.float32)
        part[...] = prod
        send1[b] = prod.astype(jnp.bfloat16)
        if b == 0:
            enter()
        for k in ahead_first(n_dp):
            to = lax.rem(dp + k, n_dp)
            push(send1.at[b, rows_of(to)], recv1.at[b, k - 1], s1.at[b], r1.at[b], at_dp(k))
        for k in ahead_first(n_dp):
            to = lax.rem(dp + k, n_dp)
            push(squares_out.at[b, to], squares_in.at[b, k - 1], s0.at[b], r0.at[b], at_dp(k))
        copies = [all_of(recv1.at[b], s1.at[b], r1.at[b]), all_of(squares_in.at[b], s0.at[b], r0.at[b])]
        total = part[rows_of(dp), :]
        all_squares = squares_out[b, dp]
        with jax.named_scope(f"wait_partials_{b}"):
            for copy in copies:
                copy.wait_recv()
        for k in range(1, n_dp):
            total = total + recv1[b, k - 1].astype(jnp.float32)
            all_squares = all_squares + squares_in[b, k - 1]
        all_squares = jnp.sum(jnp.where(spread, all_squares, 0.0), axis=1, keepdims=True)
        scale = lax.rsqrt(all_squares / model + EPS)
        proj = (scale * total).astype(jnp.bfloat16)
        query, key, value, outgate = (
            proj[:, i * dk : (i + 1) * dk].astype(jnp.float32) for i in range(4)
        )
        for copy in cell_loads if b == 0 else ():
            copy.wait()
        pre = lax.dot_general(
            proj[:, : 3 * dk], gate_w[b, 0], (((1,), (1,)), ((), ())), preferred_element_type=jnp.float32
        )
        log_input = pre[:, 0:1]
        shifted = pre[:, 1:2] + bias[:, b : b + 1]
        log_forget = jnp.minimum(shifted, 0.0) - jnp.log1p(jnp.exp(-jnp.abs(shifted)))
        old = jnp.sum(jnp.where(eye(rows), stab[b], 0.0), axis=1, keepdims=True)
        new_stab = jnp.maximum(log_forget + old, log_input)
        keep = jnp.exp(log_forget + old - new_stab)
        admit = jnp.exp(log_input - new_stab)
        scaled_key = key * dk ** (-0.5)
        admitted = admit * scaled_key
        new_norm = keep * norm[b, :, 0] + admitted
        mem_loads[b].wait()
        query_t = query.T
        recalled = jnp.concatenate(
            [
                jnp.sum(query_t[:, s : s + 1] * membuf[b, s], axis=0, keepdims=True)
                for s in range(rows)
            ],
            axis=0,
        )
        match = jnp.sum(query * admitted, axis=-1, keepdims=True)
        numer = keep * recalled + match * value
        denom = jnp.maximum(jnp.abs(jnp.sum(query * new_norm, axis=-1, keepdims=True)), 1.0)
        gated = numer / denom * jax.nn.sigmoid(outgate)
        gated = gated.astype(jnp.bfloat16)
        if b == 0:
            own_block = j
            gath[rows_of(dp), :] = gated
            for k in ahead_first(n_dp):
                push(gath.at[rows_of(dp)], gath.at[rows_of(dp)], s2.at[0], r2.at[0], at_dp(k))
            copies = [all_of(gath.at[pl.ds(0, (n_dp - 1) * rows)], s2.at[0], r2.at[0])]
        else:
            mix_copies[b].wait_recv()
            for k in range(n_dp):
                send6[b, k] = jnp.dot(
                    gated, gmix[b, k], preferred_element_type=jnp.float32
                ).astype(jnp.bfloat16)
            for k in (*ahead_first(n_dp), 0):
                to = lax.rem(dp + k, n_dp)
                turn = lax.rem(dp + to - tp + n_tp, NEAR)
                turn = jnp.where(turn > NEAR // 2, turn - NEAR, turn)
                copy = describe(
                    send6.at[b, to], recv6.at[b, turn + NEAR // 2 - 1], s6.at[b], r6.at[b],
                    {"dp": to, **at_tp(turn)},
                )
                if k:
                    copy.start()
                else:
                    pl.when(turn != 0)(copy.start)
            stays = turn == 0
            eight = describe(recv6.at[b], recv6.at[b], s6.at[b], r6.at[b], at_dp(1))
            seven = recv6.at[b, pl.ds(0, NEAR - 1)]
            seven = describe(seven, seven, s6.at[b], r6.at[b], at_dp(1))

            @pl.when(stays)
            def _():
                recv6[b, NEAR // 2 - 1] = send6[b, dp]
            own_block = lax.rem(tp - dp + n_dp, NEAR)
        vec[b, 0] = jnp.broadcast_to(keep, (rows, dk))
        vec[b, 1] = admitted
        vec[b, 2] = value
        vec[b, 3] = new_norm
        vec[b, 4] = jnp.broadcast_to(new_stab, (rows, dk))
        store(vec.at[b], vec_out.at[b])
        if b == 0:
            mix_loads[b].wait()
            with jax.named_scope(f"wait_gated_{b}"):
                for copy in copies:
                    copy.wait_recv()
            prod = jnp.dot(gath[...], mixbuf[...], preferred_element_type=jnp.float32)
            mixpart[...] = prod
            send3[...] = prod.astype(jnp.bfloat16)
            met(0, 0)
            for i, k in enumerate(window):
                to = lax.rem(tp + k + n_tp, NEAR)
                push(send3.at[rows_of(to)], recv3.at[i], s3.at[0], r3.at[0], at_tp(k))
            copies = [all_of(recv3, s3.at[0], r3.at[0])]
            mix_copies = {}
            for later in range(1, blocks):
                mix_loads[later].wait()
                for k in ahead_first(n_dp):
                    push(gmix.at[later, dp], gmix.at[later, dp], s7.at[later], r7.at[later], at_dp(k))
                mix_copies[later] = all_of(
                    gmix.at[later, pl.ds(0, n_dp - 1)], s7.at[later], r7.at[later]
                )
            total = mixpart[rows_of(j), :]
            with jax.named_scope(f"wait_near_{b}"):
                for copy in copies:
                    copy.wait_recv()
            for i in range(len(window)):
                total = total + recv3[i].astype(jnp.float32)
        else:
            with jax.named_scope(f"wait_near_{b}"):
                pl.when(stays)(seven.wait_recv)
                pl.when(jnp.logical_not(stays))(eight.wait_recv)
            total = sum(recv6[b, i].astype(jnp.float32) for i in range(NEAR))
        far[b, group] = total.astype(jnp.bfloat16)
        met(b, 1)
        for k in ahead_first(n_far):
            push(far.at[b, group], far.at[b, group], s4.at[b], r4.at[b], at_tp(NEAR * k))
        copies = [all_of(far.at[b, pl.ds(0, n_far - 1)], s4.at[b], r4.at[b])]
        total = x_now[rows_of(own_block), :].astype(jnp.float32)
        with jax.named_scope(f"wait_far_{b}"):
            for copy in copies:
                copy.wait_recv()
        mixed = far[b, 0].astype(jnp.float32)
        for k in range(1, n_far):
            mixed = mixed + far[b, k].astype(jnp.float32)
        xbuf[b, rows_of(own_block), :] = (total + mixed).astype(jnp.bfloat16)
        last = b == blocks - 1
        x_next = x_out if last else xbuf.at[b]
        for k in window:
            block = rows_of(own_block)
            push(xbuf.at[b, block], x_next.at[block], s5.at[b], r5.at[b], at_tp(k))
        copies = [all_of(x_next.at[pl.ds(0, (NEAR - 1) * rows)], s5.at[b], r5.at[b])]
        if last:
            store(xbuf.at[b, rows_of(own_block)], x_out.at[rows_of(own_block)])
        if last:
            for copy in sent[: -len(copies)]:
                copy.wait_send()
            pl.when(stays)(seven.wait_send)
            pl.when(jnp.logical_not(stays))(eight.wait_send)
            for copy in stores[:-1]:
                copy.wait()
        with jax.named_scope(f"wait_window_{b}"):
            for copy in copies:
                copy.wait_recv()
    for copy in copies:
        copy.wait_send()
    stores[-1].wait()


def finish_kernel(
    pieces, x_in, vec_in, memory_in, x_out, mem_out, norm_out, stab_out,
    x, vec, memory, fresh, new_norm, new_stab, load_sem, store_sem,
):
    blocks, rows, _, _ = memory.shape
    step = rows // pieces
    loads = [pltpu.make_async_copy(vec_in, vec, load_sem.at[0])]
    for b in range(blocks):
        for p in range(pieces):
            at = pl.ds(p * step, step)
            loads.append(
                pltpu.make_async_copy(memory_in.at[b, at, 0], memory.at[b, at], load_sem.at[len(loads)])
            )
    loads.append(pltpu.make_async_copy(x_in, x, load_sem.at[len(loads)]))
    for copy in loads:
        copy.start()
    stores = []

    def store(src, dst):
        copy = pltpu.make_async_copy(src, dst, store_sem.at[len(stores)])
        copy.start()
        stores.append(copy)

    loads[0].wait()
    for b in range(blocks):
        new_norm[b] = vec[b, 3]
        new_stab[b] = jnp.sum(jnp.where(eye(rows), vec[b, 4, :, :rows], 0.0), axis=0, keepdims=True)
        admitted_t = vec[b, 1].T
        for p in range(pieces):
            loads[1 + b * pieces + p].wait()
            for s in range(p * step, (p + 1) * step):
                fresh[b, s] = (
                    vec[b, 0, s : s + 1, :] * memory[b, s]
                    + admitted_t[:, s : s + 1] * vec[b, 2, s : s + 1, :]
                )
            at = pl.ds(p * step, step)
            store(fresh.at[b, at], mem_out.at[b, at, 0])
    loads[-1].wait()
    store(x, x_out)
    store(new_norm, norm_out.at[:, :, 0])
    store(new_stab, stab_out)
    for copy in stores:
        copy.wait()


def shards(n_dp, n_tp, *args):
    tokens, gain, wq, wk, wv, wo, gate_w, bias, wmix, memory, norm, stab = args
    blocks, rows, _, dk, _ = memory.shape
    seqs, feats = tokens.shape
    n_far = n_tp // NEAR
    dims = (blocks, rows, feats, dk, feats * n_dp)
    bf, f32 = jnp.bfloat16, jnp.float32
    gate_w, bias, stab = gate_w.transpose(0, 1, 3, 2), bias.T, stab.transpose(0, 2, 1)
    dma = pltpu.SemaphoreType.DMA
    x, vec = pl.pallas_call(
        functools.partial(step_kernel, n_dp, n_tp, dims),
        out_shape=(
            jax.ShapeDtypeStruct((seqs, feats), bf),
            jax.ShapeDtypeStruct((blocks, 5, rows, dk), f32),
        ),
        in_specs=[HBM] * 12,
        out_specs=(HBM, HBM),
        scratch_shapes=[
            *(pltpu.VMEM(a.shape, a.dtype) for a in (tokens, gain, gate_w, bias, norm, stab)),
            pltpu.VMEM((blocks, 5, rows, dk), f32),
            pltpu.VMEM((blocks, seqs, feats), bf),
            pltpu.VMEM((blocks, feats, 4 * dk), bf),
            pltpu.VMEM((dk, feats), bf),
            pltpu.VMEM((blocks, rows, dk, dk), f32),
            pltpu.VMEM((seqs, 4 * dk), f32),
            pltpu.VMEM((blocks, seqs, 4 * dk), bf),
            pltpu.VMEM((blocks, n_dp - 1, rows, 4 * dk), bf),
            pltpu.VMEM((seqs, dk), bf),
            pltpu.VMEM((seqs, feats), f32),
            pltpu.VMEM((seqs, feats), bf),
            pltpu.VMEM((NEAR - 1, rows, feats), bf),
            pltpu.VMEM((blocks, n_far, rows, feats), bf),
            pltpu.VMEM((blocks, n_dp, 1, LANES), f32),
            pltpu.VMEM((blocks, n_dp - 1, 1, LANES), f32),
            pltpu.VMEM((blocks, n_dp, dk, feats), bf),
            pltpu.VMEM((blocks, n_dp, rows, feats), bf),
            pltpu.VMEM((blocks, NEAR, rows, feats), bf),
            dma((blocks * 2 + 6,)),
            dma((blocks,)),
            dma((blocks + 1,)),
            pltpu.SemaphoreType.REGULAR((2,)),
            *(dma((blocks,)) for _ in range(8)),
            *(dma((1,)) for _ in range(4)),
            *(dma((blocks,)) for _ in range(4)),
        ],
        compiler_params=pltpu.CompilerParams(collective_id=0, has_side_effects=True),
        name="two_cells",
    )(tokens, gain, wq, wk, wv, wo, gate_w, bias, wmix, memory, norm, stab)
    pieces = 2
    copies = blocks * pieces
    x, new_memory, new_norm, new_stab = pl.pallas_call(
        functools.partial(finish_kernel, pieces),
        out_shape=(
            jax.ShapeDtypeStruct((seqs, feats), bf),
            jax.ShapeDtypeStruct(memory.shape, f32),
            jax.ShapeDtypeStruct(norm.shape, f32),
            jax.ShapeDtypeStruct(stab.shape, f32),
        ),
        in_specs=[HBM] * 3,
        out_specs=[HBM] * 4,
        scratch_shapes=[
            pltpu.VMEM((seqs, feats), bf),
            pltpu.VMEM((blocks, 5, rows, dk), f32),
            pltpu.VMEM((blocks, rows, dk, dk), f32),
            pltpu.VMEM((blocks, rows, dk, dk), f32),
            pltpu.VMEM((blocks, rows, dk), f32),
            pltpu.VMEM((blocks, 1, rows), f32),
            dma((copies + 2,)),
            dma((copies + 3,)),
        ],
        name="finish",
    )(x, vec, memory)
    return x, new_memory, new_norm, new_stab.transpose(0, 2, 1)


def solution(mesh):
    in_specs = (
        P("grp", "dp"),
        P(None, "dp"),
        P(None, "dp", "tp"),
        P(None, "dp", "tp"),
        P(None, "dp", "tp"),
        P(None, "dp", "tp"),
        P(None, "tp", None, None),
        P(None, "tp"),
        P(None, "tp", "dp"),
        P(None, ("grp", "dp"), "tp", None, None),
        P(None, ("grp", "dp"), "tp", None),
        P(None, ("grp", "dp"), "tp"),
    )
    out_specs = (
        P("grp", "dp"),
        P(None, ("grp", "dp"), "tp", None, None),
        P(None, ("grp", "dp"), "tp", None),
        P(None, ("grp", "dp"), "tp"),
    )
    body = functools.partial(shards, mesh.shape["dp"], mesh.shape["tp"])
    return jax.shard_map(body, mesh=mesh, in_specs=in_specs, out_specs=out_specs, check_vma=False)
```

```python
import functools

import jax
import jax.numpy as jnp
from jax import lax
from jax.experimental import pallas as pl
from jax.experimental.pallas import tpu as pltpu
from jax.sharding import PartitionSpec as P

EPS = 1e-06
MESH = pl.DeviceIdType.MESH
NEAR = 8
LANES = 128
HBM = pl.BlockSpec(memory_space=pltpu.HBM)
VM = pl.BlockSpec(memory_space=pltpu.VMEM)


def ahead_first(count):
    return sorted(range(1, count), key=lambda k: -min(k, count - k))


def eye(n, width=None):
    shape = (n, width or n)
    return lax.broadcasted_iota(jnp.int32, shape, 0) == lax.broadcasted_iota(jnp.int32, shape, 1)


def step_kernel(
    n_dp, n_tp, dims,
    tokens_in, gain_in, wq, wk, wv, wo, gate_in, bias_in, wmix, memory, norm_in, stab_in,
    x_out, vec_out,
    tokens, gain, gate_w, bias, norm, stab, vec, xbuf, wbuf, mixbuf, membuf, part, send1, recv1, gath, mixpart, send3, recv3, far,
    squares_out, squares_in, gmix, send6, recv6,
    load_sem, w_sem, store_sem, token, s0, r0, s7, r7, s6, r6, s1, r1, s2, r2, s3, r3, s4, r4, s5, r5,
):
    blocks, rows, feats, dk, model = dims
    cols = 4 * dk
    dp, tp = lax.axis_index("dp"), lax.axis_index("tp")
    n_far = n_tp // NEAR
    group, j = tp // NEAR, lax.rem(tp, NEAR)

    def at_dp(k):
        return {"dp": lax.rem(dp + k, n_dp)}

    def at_tp(k):
        return {"tp": lax.rem(tp + k + n_tp, n_tp)}

    window = sorted(range(-(NEAR // 2) + 1, NEAR // 2 + 1), key=lambda k: -abs(k))
    window = [k for k in window if k]

    loads = []

    def load(src, dst):
        copy = pltpu.make_async_copy(src, dst, load_sem.at[len(loads)])
        copy.start()
        loads.append(copy)
        return copy

    def load_weights(b):
        for i, w in enumerate((wq, wk, wv, wo)):
            pltpu.make_async_copy(w.at[b], wbuf.at[b, :, pl.ds(i * dk, dk)], w_sem.at[b]).start()
        return pltpu.make_async_copy(wbuf.at[b], wbuf.at[b], w_sem.at[b])

    first_loads = [load(tokens_in, tokens), load(gain_in, gain)]
    w_loads = [load_weights(0)]

    barrier = pltpu.get_barrier_semaphore()
    circles = [
        [at_tp(k) for h in range(NEAR // 2, 0, -1) for k in (h, -h)],
        [at_tp(NEAR * k) for k in ahead_first(n_far)],
    ]

    def rank(at):
        return jnp.where((at == 0) & (dp == 0), n_tp, at)

    own_rank = rank(tp)
    for k in ahead_first(n_dp):
        pl.semaphore_signal(barrier, inc=1, device_id=at_dp(k), device_id_type=MESH)
    lower, higher = jnp.int32(n_dp - 1), []
    for circle in circles:
        above = jnp.int32(0)
        for peer in circle:

            @pl.when(rank(peer["tp"]) > own_rank)
            def _(peer=peer):
                pl.semaphore_signal(barrier, inc=1, device_id=peer, device_id_type=MESH)

            above = above + jnp.where(rank(peer["tp"]) > own_rank, 1, 0)
        lower = lower + (len(circle) - above)
        higher.append(above)

    small = ((gate_in, gate_w), (bias_in, bias), (norm_in, norm), (stab_in, stab))
    cell_loads = [load(src, dst) for src, dst in small]
    mem_loads, mix_loads = [], []
    for b in range(blocks):
        if b:
            w_loads.append(load_weights(b))
        mem_loads.append(load(memory.at[b, :, 0], membuf.at[b]))
        mix_loads.append(load(wmix.at[b], gmix.at[b, dp] if b else mixbuf))

    def enter():
        with jax.named_scope("wait_barrier"):
            pl.semaphore_wait(barrier, lower)
        for i, circle in enumerate(circles):
            for peer in circle:

                @pl.when(rank(peer["tp"]) < own_rank)
                def _(peer=peer, i=i):
                    pl.semaphore_signal(token.at[i], inc=1, device_id=peer, device_id_type=MESH)

    def met(b, i):
        if b == 0:

            @pl.when(higher[i] > 0)
            def _():
                pl.semaphore_wait(token.at[i], higher[i])

    def rows_of(block):
        return pl.ds(pl.multiple_of(block * rows, rows), rows)

    sent, stores = [], []

    def store(src, dst):
        copy = pltpu.make_async_copy(src, dst, store_sem.at[len(stores)])
        copy.start()
        stores.append(copy)

    def describe(src, dst, send, recv, peer):
        return pltpu.make_async_remote_copy(
            src_ref=src, dst_ref=dst, send_sem=send, recv_sem=recv,
            device_id=peer, device_id_type=MESH,
        )

    def push(*args):
        describe(*args).start()

    def all_of(ref, send, recv):
        copy = describe(ref, ref, send, recv, at_dp(1))
        sent.append(copy)
        return copy

    for b in range(blocks):
        x_now = tokens if b == 0 else xbuf.at[b - 1]
        for copy in first_loads if b == 0 else ():
            copy.wait()
        xf = x_now[...].astype(jnp.float32)
        scaled_in = (xf * gain[b : b + 1, :]).astype(jnp.bfloat16)
        with jax.named_scope(f"wait_weights_{b}"):
            w_loads[b].wait()
        prod = jnp.dot(scaled_in, wbuf[b], preferred_element_type=jnp.float32)
        part[...] = prod
        send1[b] = prod.astype(jnp.bfloat16)
        if b == 0:
            enter()
        for k in ahead_first(n_dp):
            to = lax.rem(dp + k, n_dp)
            push(send1.at[b, rows_of(to)], recv1.at[b, k - 1], s1.at[b], r1.at[b], at_dp(k))
        squares = jnp.sum(xf * xf, axis=-1, keepdims=True)
        spread = eye(rows, LANES)
        for k in range(n_dp):
            own = jnp.where(spread, squares[k * rows : (k + 1) * rows], 0.0)
            squares_out[b, k] = jnp.sum(own, axis=0, keepdims=True)
        for k in ahead_first(n_dp):
            to = lax.rem(dp + k, n_dp)
            push(squares_out.at[b, to], squares_in.at[b, k - 1], s0.at[b], r0.at[b], at_dp(k))
        copies = [all_of(recv1.at[b], s1.at[b], r1.at[b]), all_of(squares_in.at[b], s0.at[b], r0.at[b])]
        total = part[rows_of(dp), :]
        all_squares = squares_out[b, dp]
        with jax.named_scope(f"wait_partials_{b}"):
            for copy in copies:
                copy.wait_recv()
        for k in range(1, n_dp):
            total = total + recv1[b, k - 1].astype(jnp.float32)
            all_squares = all_squares + squares_in[b, k - 1]
        all_squares = jnp.sum(jnp.where(spread, all_squares, 0.0), axis=1, keepdims=True)
        scale = lax.rsqrt(all_squares / model + EPS)
        proj = (scale * total).astype(jnp.bfloat16)
        query, key, value, outgate = (
            proj[:, i * dk : (i + 1) * dk].astype(jnp.float32) for i in range(4)
        )
        mem_loads[b].wait()
        for copy in cell_loads if b == 0 else ():
            copy.wait()
        pre = lax.dot_general(
            proj[:, : 3 * dk], gate_w[b, 0], (((1,), (1,)), ((), ())), preferred_element_type=jnp.float32
        )
        query_t = query.T
        recalled = jnp.concatenate(
            [
                jnp.sum(query_t[:, s : s + 1] * membuf[b, s], axis=0, keepdims=True)
                for s in range(rows)
            ],
            axis=0,
        )
        log_input = pre[:, 0:1]
        shifted = pre[:, 1:2] + bias[:, b : b + 1]
        log_forget = jnp.minimum(shifted, 0.0) - jnp.log1p(jnp.exp(-jnp.abs(shifted)))
        old = jnp.sum(jnp.where(eye(rows), stab[b], 0.0), axis=1, keepdims=True)
        new_stab = jnp.maximum(log_forget + old, log_input)
        keep = jnp.exp(log_forget + old - new_stab)
        admit = jnp.exp(log_input - new_stab)
        scaled_key = key * dk ** (-0.5)
        admitted = admit * scaled_key
        new_norm = keep * norm[b, :, 0] + admitted
        match = jnp.sum(query * admitted, axis=-1, keepdims=True)
        numer = keep * recalled + match * value
        denom = jnp.maximum(jnp.abs(jnp.sum(query * new_norm, axis=-1, keepdims=True)), 1.0)
        gated = numer * (1.0 / denom) * jax.nn.sigmoid(outgate)
        gated = gated.astype(jnp.bfloat16)
        if b == 0:
            own_block = j
            gath[rows_of(dp), :] = gated
            for k in ahead_first(n_dp):
                push(gath.at[rows_of(dp)], gath.at[rows_of(dp)], s2.at[0], r2.at[0], at_dp(k))
            copies = [all_of(gath.at[pl.ds(0, (n_dp - 1) * rows)], s2.at[0], r2.at[0])]
        else:
            mix_copies[b].wait_recv()
            for k in range(n_dp):
                send6[b, k] = jnp.dot(
                    gated, gmix[b, k], preferred_element_type=jnp.float32
                ).astype(jnp.bfloat16)
            for k in (*ahead_first(n_dp), 0):
                to = lax.rem(dp + k, n_dp)
                turn = lax.rem(dp + to - tp + n_tp, NEAR)
                turn = jnp.where(turn > NEAR // 2, turn - NEAR, turn)
                copy = describe(
                    send6.at[b, to], recv6.at[b, turn + NEAR // 2 - 1], s6.at[b], r6.at[b],
                    {"dp": to, **at_tp(turn)},
                )
                if k:
                    copy.start()
                else:
                    pl.when(turn != 0)(copy.start)
            stays = turn == 0
            eight = describe(recv6.at[b], recv6.at[b], s6.at[b], r6.at[b], at_dp(1))
            seven = recv6.at[b, pl.ds(0, NEAR - 1)]
            seven = describe(seven, seven, s6.at[b], r6.at[b], at_dp(1))

            @pl.when(stays)
            def _():
                recv6[b, NEAR // 2 - 1] = send6[b, dp]
            own_block = lax.rem(tp - dp + n_dp, NEAR)
        vec[b, 0] = jnp.broadcast_to(keep, (rows, dk))
        vec[b, 1] = admitted
        vec[b, 2] = value
        vec[b, 3] = new_norm
        vec[b, 4] = jnp.broadcast_to(new_stab, (rows, dk))
        store(vec.at[b], vec_out.at[b])
        if b == 0:
            mix_loads[b].wait()
            with jax.named_scope(f"wait_gated_{b}"):
                for copy in copies:
                    copy.wait_recv()
            prod = jnp.dot(gath[...], mixbuf[...], preferred_element_type=jnp.float32)
            mixpart[...] = prod
            send3[...] = prod.astype(jnp.bfloat16)
            met(0, 0)
            for i, k in enumerate(window):
                to = lax.rem(tp + k + n_tp, NEAR)
                push(send3.at[rows_of(to)], recv3.at[i], s3.at[0], r3.at[0], at_tp(k))
            copies = [all_of(recv3, s3.at[0], r3.at[0])]
            total = mixpart[rows_of(j), :]
            with jax.named_scope(f"wait_near_{b}"):
                for copy in copies:
                    copy.wait_recv()
            for i in range(len(window)):
                total = total + recv3[i].astype(jnp.float32)
        else:
            with jax.named_scope(f"wait_near_{b}"):
                pl.when(stays)(seven.wait_recv)
                pl.when(jnp.logical_not(stays))(eight.wait_recv)
            total = sum(recv6[b, i].astype(jnp.float32) for i in range(NEAR))
        far[b, group] = total.astype(jnp.bfloat16)
        met(b, 1)
        for k in ahead_first(n_far):
            push(far.at[b, group], far.at[b, group], s4.at[b], r4.at[b], at_tp(NEAR * k))
        copies = [all_of(far.at[b, pl.ds(0, n_far - 1)], s4.at[b], r4.at[b])]
        if b == 0:
            mix_copies = {}
            for later in range(1, blocks):
                mix_loads[later].wait()
                for k in ahead_first(n_dp):
                    push(gmix.at[later, dp], gmix.at[later, dp], s7.at[later], r7.at[later], at_dp(k))
                mix_copies[later] = all_of(
                    gmix.at[later, pl.ds(0, n_dp - 1)], s7.at[later], r7.at[later]
                )
        total = x_now[rows_of(own_block), :].astype(jnp.float32)
        with jax.named_scope(f"wait_far_{b}"):
            for copy in copies:
                copy.wait_recv()
        mixed = far[b, 0].astype(jnp.float32)
        for k in range(1, n_far):
            mixed = mixed + far[b, k].astype(jnp.float32)
        xbuf[b, rows_of(own_block), :] = (total + mixed).astype(jnp.bfloat16)
        last = b == blocks - 1
        x_next = x_out if last else xbuf.at[b]
        for k in window:
            block = rows_of(own_block)
            push(xbuf.at[b, block], x_next.at[block], s5.at[b], r5.at[b], at_tp(k))
        copies = [all_of(x_next.at[pl.ds(0, (NEAR - 1) * rows)], s5.at[b], r5.at[b])]
        if last:
            store(xbuf.at[b, rows_of(own_block)], x_out.at[rows_of(own_block)])
        if last:
            for copy in sent[: -len(copies)]:
                copy.wait_send()
            pl.when(stays)(seven.wait_send)
            pl.when(jnp.logical_not(stays))(eight.wait_send)
            for copy in stores[:-1]:
                copy.wait()
        with jax.named_scope(f"wait_window_{b}"):
            for copy in copies:
                copy.wait_recv()
    for copy in copies:
        copy.wait_send()
    stores[-1].wait()


def finish_kernel(
    pieces, x_in, vec_in, memory_in, x_out, mem_out, norm_out, stab_out,
    x, vec, memory, fresh, new_norm, new_stab, load_sem, store_sem,
):
    blocks, rows, _, _ = memory.shape
    step = rows // pieces
    loads = [pltpu.make_async_copy(vec_in, vec, load_sem.at[0])]
    for b in range(blocks):
        for p in range(pieces):
            at = pl.ds(p * step, step)
            loads.append(
                pltpu.make_async_copy(memory_in.at[b, at, 0], memory.at[b, at], load_sem.at[len(loads)])
            )
    loads.append(pltpu.make_async_copy(x_in, x, load_sem.at[len(loads)]))
    for copy in loads:
        copy.start()
    stores = []

    def store(src, dst):
        copy = pltpu.make_async_copy(src, dst, store_sem.at[len(stores)])
        copy.start()
        stores.append(copy)

    loads[0].wait()
    for b in range(blocks):
        new_norm[b] = vec[b, 3]
        new_stab[b] = jnp.sum(jnp.where(eye(rows), vec[b, 4, :, :rows], 0.0), axis=0, keepdims=True)
        admitted_t = vec[b, 1].T
        for p in range(pieces):
            loads[1 + b * pieces + p].wait()
            for s in range(p * step, (p + 1) * step):
                fresh[b, s] = (
                    vec[b, 0, s : s + 1, :] * memory[b, s]
                    + admitted_t[:, s : s + 1] * vec[b, 2, s : s + 1, :]
                )
            at = pl.ds(p * step, step)
            store(fresh.at[b, at], mem_out.at[b, at, 0])
    loads[-1].wait()
    store(x, x_out)
    store(new_norm, norm_out.at[:, :, 0])
    store(new_stab, stab_out)
    for copy in stores:
        copy.wait()


def shards(n_dp, n_tp, *args):
    tokens, gain, wq, wk, wv, wo, gate_w, bias, wmix, memory, norm, stab = args
    blocks, rows, _, dk, _ = memory.shape
    seqs, feats = tokens.shape
    n_far = n_tp // NEAR
    dims = (blocks, rows, feats, dk, feats * n_dp)
    bf, f32 = jnp.bfloat16, jnp.float32
    gate_w, bias, stab = gate_w.transpose(0, 1, 3, 2), bias.T, stab.transpose(0, 2, 1)
    dma = pltpu.SemaphoreType.DMA
    x, vec = pl.pallas_call(
        functools.partial(step_kernel, n_dp, n_tp, dims),
        out_shape=(
            jax.ShapeDtypeStruct((seqs, feats), bf),
            jax.ShapeDtypeStruct((blocks, 5, rows, dk), f32),
        ),
        in_specs=[HBM] * 12,
        out_specs=(HBM, HBM),
        scratch_shapes=[
            *(pltpu.VMEM(a.shape, a.dtype) for a in (tokens, gain, gate_w, bias, norm, stab)),
            pltpu.VMEM((blocks, 5, rows, dk), f32),
            pltpu.VMEM((blocks, seqs, feats), bf),
            pltpu.VMEM((blocks, feats, 4 * dk), bf),
            pltpu.VMEM((dk, feats), bf),
            pltpu.VMEM((blocks, rows, dk, dk), f32),
            pltpu.VMEM((seqs, 4 * dk), f32),
            pltpu.VMEM((blocks, seqs, 4 * dk), bf),
            pltpu.VMEM((blocks, n_dp - 1, rows, 4 * dk), bf),
            pltpu.VMEM((seqs, dk), bf),
            pltpu.VMEM((seqs, feats), f32),
            pltpu.VMEM((seqs, feats), bf),
            pltpu.VMEM((NEAR - 1, rows, feats), bf),
            pltpu.VMEM((blocks, n_far, rows, feats), bf),
            pltpu.VMEM((blocks, n_dp, 1, LANES), f32),
            pltpu.VMEM((blocks, n_dp - 1, 1, LANES), f32),
            pltpu.VMEM((blocks, n_dp, dk, feats), bf),
            pltpu.VMEM((blocks, n_dp, rows, feats), bf),
            pltpu.VMEM((blocks, NEAR, rows, feats), bf),
            dma((blocks * 2 + 6,)),
            dma((blocks,)),
            dma((blocks + 1,)),
            pltpu.SemaphoreType.REGULAR((2,)),
            *(dma((blocks,)) for _ in range(8)),
            *(dma((1,)) for _ in range(4)),
            *(dma((blocks,)) for _ in range(4)),
        ],
        compiler_params=pltpu.CompilerParams(collective_id=0, has_side_effects=True),
        name="two_cells",
    )(tokens, gain, wq, wk, wv, wo, gate_w, bias, wmix, memory, norm, stab)
    pieces = 2
    copies = blocks * pieces
    x, new_memory, new_norm, new_stab = pl.pallas_call(
        functools.partial(finish_kernel, pieces),
        out_shape=(
            jax.ShapeDtypeStruct((seqs, feats), bf),
            jax.ShapeDtypeStruct(memory.shape, f32),
            jax.ShapeDtypeStruct(norm.shape, f32),
            jax.ShapeDtypeStruct(stab.shape, f32),
        ),
        in_specs=[HBM] * 3,
        out_specs=[HBM] * 4,
        scratch_shapes=[
            pltpu.VMEM((seqs, feats), bf),
            pltpu.VMEM((blocks, 5, rows, dk), f32),
            pltpu.VMEM((blocks, rows, dk, dk), f32),
            pltpu.VMEM((blocks, rows, dk, dk), f32),
            pltpu.VMEM((blocks, rows, dk), f32),
            pltpu.VMEM((blocks, 1, rows), f32),
            dma((copies + 2,)),
            dma((copies + 3,)),
        ],
        name="finish",
    )(x, vec, memory)
    return x, new_memory, new_norm, new_stab.transpose(0, 2, 1)


def solution(mesh):
    in_specs = (
        P("grp", "dp"),
        P(None, "dp"),
        P(None, "dp", "tp"),
        P(None, "dp", "tp"),
        P(None, "dp", "tp"),
        P(None, "dp", "tp"),
        P(None, "tp", None, None),
        P(None, "tp"),
        P(None, "tp", "dp"),
        P(None, ("grp", "dp"), "tp", None, None),
        P(None, ("grp", "dp"), "tp", None),
        P(None, ("grp", "dp"), "tp"),
    )
    out_specs = (
        P("grp", "dp"),
        P(None, ("grp", "dp"), "tp", None, None),
        P(None, ("grp", "dp"), "tp", None),
        P(None, ("grp", "dp"), "tp"),
    )
    body = functools.partial(shards, mesh.shape["dp"], mesh.shape["tp"])
    return jax.shard_map(body, mesh=mesh, in_specs=in_specs, out_specs=out_specs, check_vma=False)
```

```python
import functools

import jax
import jax.numpy as jnp
from jax import lax
from jax.experimental import pallas as pl
from jax.experimental.pallas import tpu as pltpu
from jax.sharding import PartitionSpec as P

EPS = 1e-06
MESH = pl.DeviceIdType.MESH
NEAR = 8
LANES = 128
HBM = pl.BlockSpec(memory_space=pltpu.HBM)
VM = pl.BlockSpec(memory_space=pltpu.VMEM)


def ahead_first(count):
    return sorted(range(1, count), key=lambda k: -min(k, count - k))


def eye(n, width=None):
    shape = (n, width or n)
    return lax.broadcasted_iota(jnp.int32, shape, 0) == lax.broadcasted_iota(jnp.int32, shape, 1)


def step_kernel(
    n_dp, n_tp, dims,
    tokens_in, gain_in, wq, wk, wv, wo, gate_in, bias_in, wmix, memory, norm_in, stab_in,
    x_out, vec_out,
    tokens, gain, gate_w, bias, norm, stab, vec, xbuf, wbuf, mixbuf, membuf, part, send1, recv1, gath, mixpart, send3, recv3, far,
    squares_out, squares_in, gmix, send6, recv6,
    load_sem, w_sem, store_sem, token, s0, r0, s7, r7, s6, r6, s1, r1, s2, r2, s3, r3, s4, r4, s5, r5,
):
    blocks, rows, feats, dk, model = dims
    cols = 4 * dk
    dp, tp = lax.axis_index("dp"), lax.axis_index("tp")
    n_far = n_tp // NEAR
    group, j = tp // NEAR, lax.rem(tp, NEAR)

    def at_dp(k):
        return {"dp": lax.rem(dp + k, n_dp)}

    def at_tp(k):
        return {"tp": lax.rem(tp + k + n_tp, n_tp)}

    window = sorted(range(-(NEAR // 2), NEAR // 2), key=lambda k: -abs(k))
    window = [k for k in window if k]
    other = [-k for k in window]

    loads = []

    def load(src, dst):
        copy = pltpu.make_async_copy(src, dst, load_sem.at[len(loads)])
        copy.start()
        loads.append(copy)
        return copy

    def load_weights(b):
        for i, w in enumerate((wq, wk, wv, wo)):
            pltpu.make_async_copy(w.at[b], wbuf.at[b, :, pl.ds(i * dk, dk)], w_sem.at[b]).start()
        return pltpu.make_async_copy(wbuf.at[b], wbuf.at[b], w_sem.at[b])

    first_loads = [load(tokens_in, tokens), load(gain_in, gain)]
    w_loads = [load_weights(0)]

    barrier = pltpu.get_barrier_semaphore()
    circles = [
        [at_tp(k) for h in range(NEAR // 2, 0, -1) for k in (h, -h)],
        [at_tp(NEAR * k) for k in ahead_first(n_far)],
    ]

    def rank(at):
        return jnp.where((at == 0) & (dp == 0), n_tp, at)

    own_rank = rank(tp)
    for k in ahead_first(n_dp):
        pl.semaphore_signal(barrier, inc=1, device_id=at_dp(k), device_id_type=MESH)
    lower, higher = jnp.int32(n_dp - 1), []
    for circle in circles:
        above = jnp.int32(0)
        for peer in circle:

            @pl.when(rank(peer["tp"]) > own_rank)
            def _(peer=peer):
                pl.semaphore_signal(barrier, inc=1, device_id=peer, device_id_type=MESH)

            above = above + jnp.where(rank(peer["tp"]) > own_rank, 1, 0)
        lower = lower + (len(circle) - above)
        higher.append(above)

    small = ((gate_in, gate_w), (bias_in, bias), (norm_in, norm), (stab_in, stab))
    cell_loads = [load(src, dst) for src, dst in small]
    mem_loads, mix_loads = [], []
    for b in range(blocks):
        if b:
            w_loads.append(load_weights(b))
        mem_loads.append(load(memory.at[b, :, 0], membuf.at[b]))
        mix_loads.append(load(wmix.at[b], gmix.at[b, dp] if b else mixbuf))

    def enter():
        with jax.named_scope("wait_barrier"):
            pl.semaphore_wait(barrier, lower)
        for i, circle in enumerate(circles):
            for peer in circle:

                @pl.when(rank(peer["tp"]) < own_rank)
                def _(peer=peer, i=i):
                    pl.semaphore_signal(token.at[i], inc=1, device_id=peer, device_id_type=MESH)

    def met(b, i):
        if b == 0:

            @pl.when(higher[i] > 0)
            def _():
                pl.semaphore_wait(token.at[i], higher[i])

    def rows_of(block):
        return pl.ds(pl.multiple_of(block * rows, rows), rows)

    sent, stores = [], []

    def store(src, dst):
        copy = pltpu.make_async_copy(src, dst, store_sem.at[len(stores)])
        copy.start()
        stores.append(copy)

    def describe(src, dst, send, recv, peer):
        return pltpu.make_async_remote_copy(
            src_ref=src, dst_ref=dst, send_sem=send, recv_sem=recv,
            device_id=peer, device_id_type=MESH,
        )

    def push(*args):
        describe(*args).start()

    def all_of(ref, send, recv):
        copy = describe(ref, ref, send, recv, at_dp(1))
        sent.append(copy)
        return copy

    for b in range(blocks):
        x_now = tokens if b == 0 else xbuf.at[b - 1]
        for copy in first_loads if b == 0 else ():
            copy.wait()
        xf = x_now[...].astype(jnp.float32)
        scaled_in = (xf * gain[b : b + 1, :]).astype(jnp.bfloat16)
        with jax.named_scope(f"wait_weights_{b}"):
            w_loads[b].wait()
        prod = jnp.dot(scaled_in, wbuf[b], preferred_element_type=jnp.float32)
        part[...] = prod
        send1[b] = prod.astype(jnp.bfloat16)
        if b == 0:
            enter()
        for k in ahead_first(n_dp):
            to = lax.rem(dp + k, n_dp)
            push(send1.at[b, rows_of(to)], recv1.at[b, k - 1], s1.at[b], r1.at[b], at_dp(k))
        squares = jnp.sum(xf * xf, axis=-1, keepdims=True)
        spread = eye(rows, LANES)
        for k in range(n_dp):
            own = jnp.where(spread, squares[k * rows : (k + 1) * rows], 0.0)
            squares_out[b, k] = jnp.sum(own, axis=0, keepdims=True)
        for k in ahead_first(n_dp):
            to = lax.rem(dp + k, n_dp)
            push(squares_out.at[b, to], squares_in.at[b, k - 1], s0.at[b], r0.at[b], at_dp(k))
        copies = [all_of(recv1.at[b], s1.at[b], r1.at[b]), all_of(squares_in.at[b], s0.at[b], r0.at[b])]
        total = part[rows_of(dp), :]
        all_squares = squares_out[b, dp]
        with jax.named_scope(f"wait_partials_{b}"):
            for copy in copies:
                copy.wait_recv()
        for k in range(1, n_dp):
            total = total + recv1[b, k - 1].astype(jnp.float32)
            all_squares = all_squares + squares_in[b, k - 1]
        all_squares = jnp.sum(jnp.where(spread, all_squares, 0.0), axis=1, keepdims=True)
        scale = lax.rsqrt(all_squares / model + EPS)
        proj = (scale * total).astype(jnp.bfloat16)
        query, key, value, outgate = (
            proj[:, i * dk : (i + 1) * dk].astype(jnp.float32) for i in range(4)
        )
        mem_loads[b].wait()
        for copy in cell_loads if b == 0 else ():
            copy.wait()
        pre = lax.dot_general(
            proj[:, : 3 * dk], gate_w[b, 0], (((1,), (1,)), ((), ())), preferred_element_type=jnp.float32
        )
        query_t = query.T
        recalled = jnp.concatenate(
            [
                jnp.sum(query_t[:, s : s + 1] * membuf[b, s], axis=0, keepdims=True)
                for s in range(rows)
            ],
            axis=0,
        )
        log_input = pre[:, 0:1]
        shifted = pre[:, 1:2] + bias[:, b : b + 1]
        log_forget = jnp.minimum(shifted, 0.0) - jnp.log1p(jnp.exp(-jnp.abs(shifted)))
        old = jnp.sum(jnp.where(eye(rows), stab[b], 0.0), axis=1, keepdims=True)
        new_stab = jnp.maximum(log_forget + old, log_input)
        keep = jnp.exp(log_forget + old - new_stab)
        admit = jnp.exp(log_input - new_stab)
        scaled_key = key * dk ** (-0.5)
        admitted = admit * scaled_key
        new_norm = keep * norm[b, :, 0] + admitted
        match = jnp.sum(query * admitted, axis=-1, keepdims=True)
        numer = keep * recalled + match * value
        denom = jnp.maximum(jnp.abs(jnp.sum(query * new_norm, axis=-1, keepdims=True)), 1.0)
        gated = numer * (1.0 / denom) * jax.nn.sigmoid(outgate)
        gated = gated.astype(jnp.bfloat16)
        if b == 0:
            own_block = j
            gath[rows_of(dp), :] = gated
            for k in ahead_first(n_dp):
                push(gath.at[rows_of(dp)], gath.at[rows_of(dp)], s2.at[0], r2.at[0], at_dp(k))
            copies = [all_of(gath.at[pl.ds(0, (n_dp - 1) * rows)], s2.at[0], r2.at[0])]
        else:
            mix_copies[b].wait_recv()
            for k in range(n_dp):
                send6[b, k] = jnp.dot(
                    gated, gmix[b, k], preferred_element_type=jnp.float32
                ).astype(jnp.bfloat16)
            for k in (*ahead_first(n_dp), 0):
                to = lax.rem(dp + k, n_dp)
                turn = lax.rem(dp + to - tp + n_tp, NEAR)
                turn = jnp.where(turn >= NEAR // 2, turn - NEAR, turn)
                copy = describe(
                    send6.at[b, to], recv6.at[b, turn + NEAR // 2], s6.at[b - 1], r6.at[b - 1],
                    {"dp": to, **at_tp(turn)},
                )
                if k:
                    copy.start()
                else:
                    pl.when(turn != 0)(copy.start)
            stays = turn == 0
            eight = describe(recv6.at[b], recv6.at[b], s6.at[b - 1], r6.at[b - 1], at_dp(1))
            seven = recv6.at[b, pl.ds(0, NEAR - 1)]
            seven = describe(seven, seven, s6.at[b - 1], r6.at[b - 1], at_dp(1))

            @pl.when(stays)
            def _():
                recv6[b, NEAR // 2] = send6[b, dp]
            own_block = lax.rem(tp - dp + n_dp, NEAR)
        vec[b, 0] = jnp.broadcast_to(keep, (rows, dk))
        vec[b, 1] = admitted
        vec[b, 2] = value
        vec[b, 3] = new_norm
        vec[b, 4] = jnp.broadcast_to(new_stab, (rows, dk))
        store(vec.at[b], vec_out.at[b])
        if b == 0:
            mix_loads[b].wait()
            with jax.named_scope(f"wait_gated_{b}"):
                for copy in copies:
                    copy.wait_recv()
            prod = jnp.dot(gath[...], mixbuf[...], preferred_element_type=jnp.float32)
            mixpart[...] = prod
            send3[...] = prod.astype(jnp.bfloat16)
            met(0, 0)
            for i, k in enumerate(window):
                to = lax.rem(tp + k + n_tp, NEAR)
                push(send3.at[rows_of(to)], recv3.at[i], s3.at[0], r3.at[0], at_tp(k))
            copies = [all_of(recv3, s3.at[0], r3.at[0])]
            total = mixpart[rows_of(j), :]
            with jax.named_scope(f"wait_near_{b}"):
                for copy in copies:
                    copy.wait_recv()
            for i in range(len(window)):
                total = total + recv3[i].astype(jnp.float32)
        else:
            with jax.named_scope(f"wait_near_{b}"):
                pl.when(stays)(seven.wait_recv)
                pl.when(jnp.logical_not(stays))(eight.wait_recv)
            total = sum(recv6[b, i].astype(jnp.float32) for i in range(NEAR))
        far[b, group] = total.astype(jnp.bfloat16)
        met(b, 1)
        for k in ahead_first(n_far):
            push(far.at[b, group], far.at[b, group], s4.at[b], r4.at[b], at_tp(NEAR * k))
        copies = [all_of(far.at[b, pl.ds(0, n_far - 1)], s4.at[b], r4.at[b])]
        if b == 0:
            mix_copies = {}
            for later in range(1, blocks):
                mix_loads[later].wait()
                for k in ahead_first(n_dp):
                    push(gmix.at[later, dp], gmix.at[later, dp], s7.at[later - 1], r7.at[later - 1], at_dp(k))
                mix_copies[later] = all_of(
                    gmix.at[later, pl.ds(0, n_dp - 1)], s7.at[later - 1], r7.at[later - 1]
                )
        total = x_now[rows_of(own_block), :].astype(jnp.float32)
        with jax.named_scope(f"wait_far_{b}"):
            for copy in copies:
                copy.wait_recv()
        mixed = far[b, 0].astype(jnp.float32)
        for k in range(1, n_far):
            mixed = mixed + far[b, k].astype(jnp.float32)
        xbuf[b, rows_of(own_block), :] = (total + mixed).astype(jnp.bfloat16)
        last = b == blocks - 1
        x_next = x_out if last else xbuf.at[b]
        for k in (other if last else window):
            block = rows_of(own_block)
            push(xbuf.at[b, block], x_next.at[block], s5.at[b], r5.at[b], at_tp(k))
        copies = [all_of(x_next.at[pl.ds(0, (NEAR - 1) * rows)], s5.at[b], r5.at[b])]
        if last:
            store(xbuf.at[b, rows_of(own_block)], x_out.at[rows_of(own_block)])
        if last:
            for copy in sent[: -len(copies)]:
                copy.wait_send()
            pl.when(stays)(seven.wait_send)
            pl.when(jnp.logical_not(stays))(eight.wait_send)
            for copy in stores[:-1]:
                copy.wait()
        with jax.named_scope(f"wait_window_{b}"):
            for copy in copies:
                copy.wait_recv()
    for copy in copies:
        copy.wait_send()
    stores[-1].wait()


def finish_kernel(
    pieces, x_in, vec_in, memory_in, x_out, mem_out, norm_out, stab_out,
    x, vec, memory, fresh, new_norm, new_stab, load_sem, store_sem,
):
    blocks, rows, _, _ = memory.shape
    step = rows // pieces
    loads = [pltpu.make_async_copy(vec_in, vec, load_sem.at[0])]
    for b in range(blocks):
        for p in range(pieces):
            at = pl.ds(p * step, step)
            loads.append(
                pltpu.make_async_copy(memory_in.at[b, at, 0], memory.at[b, at], load_sem.at[len(loads)])
            )
    loads.append(pltpu.make_async_copy(x_in, x, load_sem.at[len(loads)]))
    for copy in loads:
        copy.start()
    stores = []

    def store(src, dst):
        copy = pltpu.make_async_copy(src, dst, store_sem.at[len(stores)])
        copy.start()
        stores.append(copy)

    loads[0].wait()
    for b in range(blocks):
        new_norm[b] = vec[b, 3]
        new_stab[b] = jnp.sum(jnp.where(eye(rows), vec[b, 4, :, :rows], 0.0), axis=0, keepdims=True)
        admitted_t = vec[b, 1].T
        for p in range(pieces):
            loads[1 + b * pieces + p].wait()
            for s in range(p * step, (p + 1) * step):
                fresh[b, s] = (
                    vec[b, 0, s : s + 1, :] * memory[b, s]
                    + admitted_t[:, s : s + 1] * vec[b, 2, s : s + 1, :]
                )
            at = pl.ds(p * step, step)
            store(fresh.at[b, at], mem_out.at[b, at, 0])
    loads[-1].wait()
    store(x, x_out)
    store(new_norm, norm_out.at[:, :, 0])
    store(new_stab, stab_out)
    for copy in stores:
        copy.wait()


def shards(n_dp, n_tp, *args):
    tokens, gain, wq, wk, wv, wo, gate_w, bias, wmix, memory, norm, stab = args
    blocks, rows, _, dk, _ = memory.shape
    seqs, feats = tokens.shape
    n_far = n_tp // NEAR
    dims = (blocks, rows, feats, dk, feats * n_dp)
    bf, f32 = jnp.bfloat16, jnp.float32
    gate_w, bias, stab = gate_w.transpose(0, 1, 3, 2), bias.T, stab.transpose(0, 2, 1)
    dma = pltpu.SemaphoreType.DMA
    x, vec = pl.pallas_call(
        functools.partial(step_kernel, n_dp, n_tp, dims),
        out_shape=(
            jax.ShapeDtypeStruct((seqs, feats), bf),
            jax.ShapeDtypeStruct((blocks, 5, rows, dk), f32),
        ),
        in_specs=[HBM] * 12,
        out_specs=(HBM, HBM),
        scratch_shapes=[
            *(pltpu.VMEM(a.shape, a.dtype) for a in (tokens, gain, gate_w, bias, norm, stab)),
            pltpu.VMEM((blocks, 5, rows, dk), f32),
            pltpu.VMEM((blocks, seqs, feats), bf),
            pltpu.VMEM((blocks, feats, 4 * dk), bf),
            pltpu.VMEM((dk, feats), bf),
            pltpu.VMEM((blocks, rows, dk, dk), f32),
            pltpu.VMEM((seqs, 4 * dk), f32),
            pltpu.VMEM((blocks, seqs, 4 * dk), bf),
            pltpu.VMEM((blocks, n_dp - 1, rows, 4 * dk), bf),
            pltpu.VMEM((seqs, dk), bf),
            pltpu.VMEM((seqs, feats), f32),
            pltpu.VMEM((seqs, feats), bf),
            pltpu.VMEM((NEAR - 1, rows, feats), bf),
            pltpu.VMEM((blocks, n_far, rows, feats), bf),
            pltpu.VMEM((blocks, n_dp, 1, LANES), f32),
            pltpu.VMEM((blocks, n_dp - 1, 1, LANES), f32),
            pltpu.VMEM((blocks, n_dp, dk, feats), bf),
            pltpu.VMEM((blocks, n_dp, rows, feats), bf),
            pltpu.VMEM((blocks, NEAR, rows, feats), bf),
            dma((blocks * 2 + 6,)),
            dma((blocks,)),
            dma((blocks + 1,)),
            pltpu.SemaphoreType.REGULAR((2,)),
            *(dma((blocks,)) for _ in range(2)),
            *(dma((blocks - 1,)) for _ in range(4)),
            *(dma((blocks,)) for _ in range(2)),
            *(dma((1,)) for _ in range(4)),
            *(dma((blocks,)) for _ in range(4)),
        ],
        compiler_params=pltpu.CompilerParams(collective_id=0, has_side_effects=True),
        name="two_cells",
    )(tokens, gain, wq, wk, wv, wo, gate_w, bias, wmix, memory, norm, stab)
    pieces = 2
    copies = blocks * pieces
    x, new_memory, new_norm, new_stab = pl.pallas_call(
        functools.partial(finish_kernel, pieces),
        out_shape=(
            jax.ShapeDtypeStruct((seqs, feats), bf),
            jax.ShapeDtypeStruct(memory.shape, f32),
            jax.ShapeDtypeStruct(norm.shape, f32),
            jax.ShapeDtypeStruct(stab.shape, f32),
        ),
        in_specs=[HBM] * 3,
        out_specs=[HBM] * 4,
        scratch_shapes=[
            pltpu.VMEM((seqs, feats), bf),
            pltpu.VMEM((blocks, 5, rows, dk), f32),
            pltpu.VMEM((blocks, rows, dk, dk), f32),
            pltpu.VMEM((blocks, rows, dk, dk), f32),
            pltpu.VMEM((blocks, rows, dk), f32),
            pltpu.VMEM((blocks, 1, rows), f32),
            dma((copies + 2,)),
            dma((copies + 3,)),
        ],
        name="finish",
    )(x, vec, memory)
    return x, new_memory, new_norm, new_stab.transpose(0, 2, 1)


def solution(mesh):
    in_specs = (
        P("grp", "dp"),
        P(None, "dp"),
        P(None, "dp", "tp"),
        P(None, "dp", "tp"),
        P(None, "dp", "tp"),
        P(None, "dp", "tp"),
        P(None, "tp", None, None),
        P(None, "tp"),
        P(None, "tp", "dp"),
        P(None, ("grp", "dp"), "tp", None, None),
        P(None, ("grp", "dp"), "tp", None),
        P(None, ("grp", "dp"), "tp"),
    )
    out_specs = (
        P("grp", "dp"),
        P(None, ("grp", "dp"), "tp", None, None),
        P(None, ("grp", "dp"), "tp", None),
        P(None, ("grp", "dp"), "tp"),
    )
    body = functools.partial(shards, mesh.shape["dp"], mesh.shape["tp"])
    return jax.shard_map(body, mesh=mesh, in_specs=in_specs, out_specs=out_specs, check_vma=False)
```
